512 devices in a mesh: fs: 64 (over z, y), tp: 8 (over x, core).
Axes of the slice: x: 4, y: 8, z: 8, core: 2. Of those that a mesh axis runs over, the one named last changes fastest.
Arguments:
- inputs: bfloat16 [24576, 2048], P('fs'), may hold values from -6 to 6
- gain: float32 [2048], replicated, may hold values from 0.1 to 1.9
- w_gate: bfloat16 [2048, 2816], P('fs', 'tp'), may hold values from -0.125 to 0.125
- w_up: bfloat16 [2048, 2816], P('fs', 'tp'), may hold values from -0.125 to 0.125
- w_down: bfloat16 [2816, 2048], P('tp', 'fs'), may hold values from -0.109375 to 0.109375
- cotangent: bfloat16 [24576, 2048], P('fs'), may hold values from -16 to 16
Outputs:
- input_gradient: bfloat16 [24576, 2048], P('fs')
- grad_down: float32 [2816, 2048], P('tp', 'fs')
The draws below stay inside these ranges and needn't reach their ends.
All inputs are finite; a program needn't handle non-finite values.
Results may differ from the reference program's by a relative error of at most 0.014.
Values may be sent and summed in bfloat16 or wider, within the bound.
No kernel may reach another device: no remote copies, remote signals or barrier semaphores. Data moves between devices by JAX's collectives and lax.ppermute only.
A program may use at most 64 MiB of HBM per device.

```python
import jax
import jax.numpy as jnp
from jax import lax

D = 2048
HID = 2816
TOKENS = 24576
N_TP = 8


def with_spikes(result, own_key, source, target, blocks, factor):
    owner, partner = [(jnp.arange(result.shape[axis_at]) // (result.shape[axis_at] // blocks)).reshape([-1 if axis == axis_at else 1 for axis in range(result.ndim)]) for axis_at in (source, target)]
    chosen = jax.random.permutation(own_key, blocks)[partner]
    strong = (owner == chosen) | (owner == (partner + blocks // 2) % blocks)
    return jnp.where(strong, factor * result, result)


def shard_levels(own_key, shape, split, low, largest):
    level = 1.0
    for dim, shards_of in split:
        heights = jax.random.uniform(jax.random.fold_in(jax.random.fold_in(own_key, 6), dim), (shards_of,), jnp.float32, low / len(split), largest / len(split))
        level = level * jnp.repeat(jnp.exp(heights), shape[dim] // shards_of).reshape((-1,) + (1,) * (len(shape) - 1 - dim))
    return level


def noise(key, dims, spread, reach, shards=(), dtype=jnp.bfloat16):
    result = jax.random.normal(key, dims, jnp.float32) * spread
    if len(shards) > 0:
        result = shard_levels(key, dims, shards, -0.22, 0.18) * result
    return jnp.clip(result, min=-reach, max=reach).astype(dtype)


def gaussian_with(rng, shape, scale, most, cuts, heavy, kind=jnp.bfloat16):
    values = scale * jax.random.normal(rng, shape, jnp.float32)
    if cuts:
        values = values * shard_levels(rng, shape, cuts, -0.22, 0.18)
    return jnp.clip(with_spikes(values, jax.random.fold_in(rng, 3), *heavy), -most, most).astype(kind)


def setup_inputs(seed: int = 0) -> dict:
    seeds = jax.random.split(jax.random.key(seed), 7)
    inputs = noise(seeds[0], (TOKENS, D), 1.0, 6.0, ((0, 64),))
    gain = jnp.clip(1.0 + 0.18 * jax.random.normal(seeds[1], (D,), jnp.float32), 0.1, 1.9)
    w_gate = noise(seeds[2], (D, HID), D ** -0.5, 0.125, ((0, 64), (1, 8)))
    w_up = noise(seeds[3], (D, HID), D ** -0.5, 0.125, ((0, 64), (1, 8)))
    w_down = noise(seeds[4], (HID, D), HID ** -0.5, 0.109375, ((0, 8), (1, 64)))
    cotangent = gaussian_with(seeds[5], (TOKENS, D), 1.0, 16.0, ((0, 64),), (0, 1, 64, 4.0))
    return dict(inputs=inputs, gain=gain, w_gate=w_gate, w_up=w_up, w_down=w_down, cotangent=cotangent)


EPSILON = 1e-06
HALF_STEP = 0.5

def reference(inputs, gain, w_gate, w_up, w_down, cotangent):
    value_entries = inputs.astype(jnp.float32)
    inverse_norm_factor = lax.rsqrt(lax.optimization_barrier(jnp.mean(value_entries * value_entries, axis=-1, keepdims=True)) + EPSILON)
    normalized_input = value_entries * inverse_norm_factor
    normalized_rows = (normalized_input * gain.astype(jnp.float32)).astype(jnp.bfloat16)
    gate_value = jnp.dot(normalized_rows, w_gate, preferred_element_type=jnp.float32)
    up_projection_value = jnp.dot(normalized_rows, w_up, preferred_element_type=jnp.float32)
    sigmoid_gate = jax.nn.sigmoid(gate_value)
    hidden = (gate_value * sigmoid_gate * up_projection_value).astype(jnp.bfloat16)
    d_hidden = HALF_STEP * jnp.dot(cotangent, w_down.T, preferred_element_type=jnp.float32)
    grad_down = HALF_STEP * jnp.dot(hidden.T, cotangent, preferred_element_type=jnp.float32)
    d_gate = (d_hidden * up_projection_value * sigmoid_gate * (1.0 + gate_value * (1.0 - sigmoid_gate))).astype(jnp.bfloat16)
    d_up = (d_hidden * gate_value * sigmoid_gate).astype(jnp.bfloat16)
    block_width = HID // N_TP
    d_normed = jnp.zeros(value_entries.shape, jnp.float32)
    for block in range(N_TP):
        lower = block * block_width
        upper = lower + block_width
        partial_term = jnp.dot(d_gate[:, lower:upper], w_gate[:, lower:upper].T, preferred_element_type=jnp.float32)
        partial_term = partial_term + jnp.dot(d_up[:, lower:upper], w_up[:, lower:upper].T, preferred_element_type=jnp.float32)
        rounded = lax.optimization_barrier(partial_term.astype(jnp.bfloat16))
        d_normed = d_normed + rounded.astype(jnp.float32)
    scaled_hidden = d_normed * gain.astype(jnp.float32)
    input_gradient = inverse_norm_factor * (scaled_hidden - normalized_input * lax.optimization_barrier(jnp.mean(scaled_hidden * normalized_input, axis=-1, keepdims=True)))
    return (input_gradient.astype(jnp.bfloat16), grad_down)
```

```python
import jax
import jax.numpy as jnp
from jax import lax
from jax.experimental import pallas as pl
from jax.experimental.pallas import tpu as pltpu
from jax.sharding import Mesh
from jax.sharding import PartitionSpec as P

AXES = ("z", "y", "x", "c")
NZ, NY, NX, NC = 8, 8, 4, 2
FS = ("z", "y")
TP = ("x", "c")
EPSILON = 1e-06
HALF_STEP = 0.5
TOK = 384
D = 2048
HU = 352
HP = 384
DROWS = 32


def device_number(z, y, x, c):
    return ((z % NZ * NY + y % NY) * NX + x) * NC + c


def ring_pairs(step):
    return [
        (device_number(z, y, x, c), device_number(z + (1 - c) * step, y + c * step, x, c))
        for z in range(NZ)
        for y in range(NY)
        for x in range(NX)
        for c in range(NC)
    ]


def line_groups(along_ring):
    groups = []
    for x in range(NX):
        for c in range(NC):
            vary_z = (c == 0) == along_ring
            for fixed in range(8):
                groups.append(
                    [
                        device_number(k, fixed, x, c) if vary_z else device_number(fixed, k, x, c)
                        for k in range(8)
                    ]
                )
    return groups


def ring(array, step):
    return lax.ppermute(array, AXES, ring_pairs(step))


def exchange(array, along_ring):
    return lax.all_to_all(
        array, AXES, 0, 0, axis_index_groups=line_groups(along_ring), tiled=True
    )


def dot(left, right, dims):
    return lax.dot_general(left, right, (dims, ((), ())), preferred_element_type=jnp.float32)


def compute_kernel(
    place, x_ref, gain_ref, cot_ref, b0, f1, f2, f3, g1, g2, g3, f4, g4,
    keep_ref, send_ref, down_ref, w_ref, xn_ref, dt_ref,
):
    r = place[0]
    c = place[1]

    def row_of(q, o):
        q = lax.rem(q + 16, 8)
        return pl.multiple_of(jnp.where(c == 0, q * 256 + o * 32, o * 256 + q * 32), 32)

    def put(q, block, first, last):
        for o in range(first, last):
            w_ref[pl.ds(row_of(q, o), DROWS), :] = block[pl.ds((o - first) * DROWS, DROWS), :]

    put(r, b0, 0, 8)
    put(r - 1, f1, 0, 8)
    put(r - 2, f2, 0, 8)
    put(r - 3, f3, 0, 8)
    put(r + 1, g1, 0, 8)
    put(r + 2, g2, 0, 8)
    put(r + 3, g3, 0, 8)
    put(r - 4, f4, 0, 4)
    put(r - 4, g4, 4, 8)

    gain = gain_ref[...]
    for k in range(6):
        rows = pl.ds(k * 64, 64)
        value = x_ref[rows, :].astype(jnp.float32)
        inverse = lax.rsqrt(jnp.mean(value * value, axis=-1, keepdims=True) + EPSILON)
        xn_ref[rows, :] = (value * inverse * gain).astype(jnp.bfloat16)

    gate_up = dot(xn_ref[...], w_ref[:, : 2 * HP], ((1,), (0,)))
    gate = gate_up[:, :HP]
    up = gate_up[:, HP:]
    d_hidden = HALF_STEP * dot(cot_ref[...], w_ref[:, 2 * HP :], ((1,), (0,)))
    sig = jax.nn.sigmoid(gate)
    hidden = (gate * sig * up).astype(jnp.bfloat16)
    d_gate = (d_hidden * up * sig * (1.0 + gate * (1.0 - sig))).astype(jnp.bfloat16)
    d_up = (d_hidden * gate * sig).astype(jnp.bfloat16)
    both = jnp.concatenate([d_gate, d_up], axis=1)
    xn_ref[...] = dot(both, w_ref[:, : 2 * HP], ((1,), (1,))).astype(jnp.bfloat16)
    half = TOK // 2
    keep_ref[...] = xn_ref[pl.ds(pl.multiple_of(c * half, 64), half), :]
    send_ref[...] = xn_ref[pl.ds(pl.multiple_of((1 - c) * half, 64), half), :]
    dt_ref[...] = (HALF_STEP * dot(cot_ref[...], hidden, ((0,), (0,)))).astype(jnp.bfloat16)
    for q in range(8):
        for o in range(8):
            down_ref[pl.ds(q * 256 + o * 32, DROWS), :] = dt_ref[pl.ds(row_of(q, o), DROWS), :]


def compute(place, inputs, gain, cotangent, blocks):
    vmem = pl.BlockSpec(memory_space=pltpu.VMEM)
    return pl.pallas_call(
        compute_kernel,
        out_shape=(
            jax.ShapeDtypeStruct((TOK // 2, D), jnp.bfloat16),
            jax.ShapeDtypeStruct((TOK // 2, D), jnp.bfloat16),
            jax.ShapeDtypeStruct((D, HP), jnp.bfloat16),
        ),
        in_specs=[pl.BlockSpec(memory_space=pltpu.SMEM)] + [vmem] * 12,
        out_specs=(vmem,) * 3,
        scratch_shapes=[
            pltpu.VMEM((D, 3 * HP), jnp.bfloat16),
            pltpu.VMEM((TOK, D), jnp.bfloat16),
            pltpu.VMEM((D, HP), jnp.bfloat16),
        ],
        compiler_params=pltpu.CompilerParams(vmem_limit_bytes=48 * 2**20),
    )(place, inputs, gain.reshape(1, D), cotangent, *blocks)


def shards(inputs, gain, w_gate, w_up, w_down, cotangent):
    z, y, x, c = (lax.axis_index(a) for a in AXES)
    r = jnp.where(c == 0, z, y)
    place = jnp.stack([r, c]).astype(jnp.int32)

    pad = ((0, 0), (0, HP - HU))
    packed = jnp.concatenate([jnp.pad(w, pad) for w in (w_gate, w_up, w_down.T)], axis=1)
    b0 = exchange(jnp.broadcast_to(packed[None], (8, DROWS, 3 * HP)), False)
    b0 = b0.reshape(256, 3 * HP)
    f1 = ring(b0, 1)
    g1 = ring(b0, -1)
    f2 = ring(f1, 1)
    g2 = ring(g1, -1)
    f3 = ring(f2, 1)
    g3 = ring(g2, -1)
    f4 = ring(f3[:128], 1)
    g4 = ring(g3[128:], -1)

    keep, send, down = compute(place, inputs, gain, cotangent, (b0, f1, f2, f3, g1, g2, g3, f4, g4))

    arrived = exchange(down.reshape(8, 256, HP), True)
    line = arrived.astype(jnp.float32).sum(axis=0).astype(jnp.bfloat16)
    arrived = exchange(line.reshape(8, DROWS, HP), False)
    grad_down = arrived.astype(jnp.float32).sum(axis=0)[:, :HU].T

    other = lax.ppermute(send, "c", [(0, 1), (1, 0)])
    pair = (keep.astype(jnp.float32) + other.astype(jnp.float32)).astype(jnp.bfloat16)
    quarters = lax.all_to_all(pair.reshape(4, TOK // 8, D), "x", 0, 0, tiled=True)
    d_normed = quarters.astype(jnp.float32).sum(axis=0)
    value = lax.dynamic_slice_in_dim(inputs, c * (TOK // 2) + x * (TOK // 8), TOK // 8, 0)
    value = value.astype(jnp.float32)
    inverse = lax.rsqrt(jnp.mean(value * value, axis=-1, keepdims=True) + EPSILON)
    normalized = value * inverse
    scaled = d_normed * gain
    mine = inverse * (
        scaled - normalized * jnp.mean(scaled * normalized, axis=-1, keepdims=True)
    )
    mine = mine.astype(jnp.bfloat16)
    half = lax.all_gather(mine, "x", axis=0, tiled=True)
    whole = lax.all_to_all(
        jnp.broadcast_to(half[None], (2, TOK // 2, D)), "c", 0, 0, tiled=True
    )
    return whole.reshape(TOK, D), grad_down


def solution(mesh):
    split = Mesh(mesh.devices.reshape(NZ, NY, NX, NC), AXES)
    in_specs = (P(FS, None), P(), P(FS, TP), P(FS, TP), P(TP, FS), P(FS, None))
    out_specs = (P(FS, None), P(TP, FS))
    return jax.shard_map(
        shards, mesh=split, in_specs=in_specs, out_specs=out_specs, check_vma=False
    )
```

```python
import jax
import jax.numpy as jnp
from jax import lax
from jax.experimental import pallas as pl
from jax.experimental.pallas import tpu as pltpu
from jax.sharding import Mesh
from jax.sharding import PartitionSpec as P

AXES = ("z", "y", "x", "c")
NZ, NY, NX, NC = 8, 8, 4, 2
FS = ("z", "y")
TP = ("x", "c")
EPSILON = 1e-06
HALF_STEP = 0.5
TOK = 384
D = 2048
HU = 352
HP = 384
DROWS = 32
HALF = TOK // NC
QUARTER = HALF // NX
VMEM_LIMIT = 32 * 2**20
SMALL_LIMIT = 10 * 2**20


def device_number(z, y, x, c):
    return ((z % NZ * NY + y % NY) * NX + x) * NC + c


def ring_pairs(step):
    return [
        (device_number(z, y, x, c), device_number(z + (1 - c) * step, y + c * step, x, c))
        for z in range(NZ)
        for y in range(NY)
        for x in range(NX)
        for c in range(NC)
    ]


def line_groups(along_ring):
    groups = []
    for x in range(NX):
        for c in range(NC):
            vary_z = (c == 0) == along_ring
            for fixed in range(8):
                groups.append(
                    [
                        device_number(k, fixed, x, c) if vary_z else device_number(fixed, k, x, c)
                        for k in range(8)
                    ]
                )
    return groups


def ring(array, step):
    return lax.ppermute(array, AXES, ring_pairs(step))


def exchange(array, along_ring):
    return lax.all_to_all(
        array, AXES, 0, 0, axis_index_groups=line_groups(along_ring), tiled=True
    )


def dot(left, right, dims):
    return lax.dot_general(left, right, (dims, ((), ())), preferred_element_type=jnp.float32)


def compute_kernel(
    x_ref, gain_ref, cot_ref, a0, a1, a2, a3, a4, b1, b2, b3,
    p0, p1, p2, p3, m1, m2, m3, m4,
    own_ref, k1_ref, k2_ref, k3_ref, send_ref, x_own_ref, down_ref, w_ref, xn_ref, dt_ref,
):
    x = lax.axis_index("x")
    c = lax.axis_index("c")
    r = jnp.where(c == 0, lax.axis_index("z"), lax.axis_index("y"))

    def row_of(q, o):
        q = lax.rem(q + 16, 8)
        return pl.multiple_of(jnp.where(c == 0, q * 256 + o * 32, o * 256 + q * 32), 32)

    def put(q, block, first):
        for o in range(4):
            w_ref[pl.ds(row_of(q, o + first), DROWS), :] = block[pl.ds(o * DROWS, DROWS), :]

    for k, block in enumerate((a0, a1, a2, a3, a4)):
        put(r - k, block, 0)
    for k, block in enumerate((b1, b2, b3)):
        put(r + k + 1, block, 0)
    for k, block in enumerate((p0, p1, p2, p3)):
        put(r - k, block, 4)
    for k, block in enumerate((m1, m2, m3, m4)):
        put(r + k + 1, block, 4)

    gain = gain_ref[...]
    for k in range(6):
        rows = pl.ds(k * 64, 64)
        value = x_ref[rows, :].astype(jnp.float32)
        inverse = lax.rsqrt(jnp.mean(value * value, axis=-1, keepdims=True) + EPSILON)
        xn_ref[rows, :] = (value * inverse * gain).astype(jnp.bfloat16)

    gate_up = dot(xn_ref[...], w_ref[:, : 2 * HP], ((1,), (0,)))
    gate = gate_up[:, :HP]
    up = gate_up[:, HP:]
    d_hidden = HALF_STEP * dot(cot_ref[...], w_ref[:, 2 * HP :], ((1,), (0,)))
    sig = jax.nn.sigmoid(gate)
    hidden = (gate * sig * up).astype(jnp.bfloat16)
    d_gate = (d_hidden * up * sig * (1.0 + gate * (1.0 - sig))).astype(jnp.bfloat16)
    d_up = (d_hidden * gate * sig).astype(jnp.bfloat16)
    both = jnp.concatenate([d_gate, d_up], axis=1)
    xn_ref[...] = dot(both, w_ref[:, : 2 * HP], ((1,), (1,))).astype(jnp.bfloat16)

    def quarter(core, k):
        row = core * HALF + lax.rem(x + k, NX) * QUARTER
        return pl.ds(pl.multiple_of(row, 16), QUARTER)

    for k, ref in enumerate((own_ref, k1_ref, k2_ref, k3_ref)):
        ref[...] = xn_ref[quarter(c, k), :]
        send_ref[pl.ds(k * QUARTER, QUARTER), :] = xn_ref[quarter(1 - c, k), :]
    x_own_ref[...] = x_ref[quarter(c, 0), :]
    dt_ref[...] = (HALF_STEP * dot(cot_ref[...], hidden, ((0,), (0,)))).astype(jnp.bfloat16)
    for q in range(8):
        for o in range(8):
            down_ref[pl.ds(q * 256 + o * 32, DROWS), :] = dt_ref[pl.ds(row_of(q, o), DROWS), :]


def vmem_specs(count):
    return [pl.BlockSpec(memory_space=pltpu.VMEM)] * count


def small_call(kernel, out_shape, *operands):
    count = len(out_shape)
    return pl.pallas_call(
        kernel,
        out_shape=tuple(out_shape),
        in_specs=vmem_specs(len(operands)),
        out_specs=tuple(vmem_specs(count)),
        compiler_params=pltpu.CompilerParams(vmem_limit_bytes=SMALL_LIMIT),
    )(*operands)


def compute(inputs, gain, cotangent, blocks):
    quarter = jax.ShapeDtypeStruct((QUARTER, D), jnp.bfloat16)
    return pl.pallas_call(
        compute_kernel,
        out_shape=(
            quarter, quarter, quarter, quarter,
            jax.ShapeDtypeStruct((HALF, D), jnp.bfloat16),
            quarter,
            jax.ShapeDtypeStruct((D, HP), jnp.bfloat16),
        ),
        in_specs=vmem_specs(3 + len(blocks)),
        out_specs=tuple(vmem_specs(7)),
        scratch_shapes=[
            pltpu.VMEM((D, 3 * HP), jnp.bfloat16),
            pltpu.VMEM((TOK, D), jnp.bfloat16),
            pltpu.VMEM((D, HP), jnp.bfloat16),
        ],
        compiler_params=pltpu.CompilerParams(vmem_limit_bytes=VMEM_LIMIT),
    )(inputs, gain.reshape(1, D), cotangent, *blocks)


def pair_kernel(own_ref, k1_ref, k2_ref, k3_ref, other_ref, s0_ref, s1_ref, s2_ref, s3_ref):
    kept = (own_ref, k1_ref, k2_ref, k3_ref)
    for k, out in enumerate((s0_ref, s1_ref, s2_ref, s3_ref)):
        other = other_ref[pl.ds(k * QUARTER, QUARTER), :].astype(jnp.float32)
        out[...] = (kept[k][...].astype(jnp.float32) + other).astype(out.dtype)


def final_kernel(x_ref, gain_ref, own_ref, q1_ref, q2_ref, q3_ref, out_ref):
    value = x_ref[...].astype(jnp.float32)
    inverse = lax.rsqrt(jnp.mean(value * value, axis=-1, keepdims=True) + EPSILON)
    normalized = value * inverse
    d_normed = own_ref[...]
    for ref in (q1_ref, q2_ref, q3_ref):
        d_normed = d_normed + ref[...].astype(jnp.float32)
    scaled = d_normed * gain_ref[...]
    mean = jnp.mean(scaled * normalized, axis=-1, keepdims=True)
    out_ref[...] = (inverse * (scaled - normalized * mean)).astype(jnp.bfloat16)


def sum_kernel(parts_ref, out_ref):
    total = parts_ref[0].astype(jnp.float32)
    for k in range(1, 8):
        total = total + parts_ref[k].astype(jnp.float32)
    out_ref[...] = total.astype(out_ref.dtype)


def along_x(array, step):
    return lax.ppermute(array, "x", [(k, (k + step) % NX) for k in range(NX)])


def shards(inputs, gain, w_gate, w_up, w_down, cotangent):
    c = lax.axis_index("c")
    pad = ((0, 0), (0, HP - HU))
    packed = jnp.concatenate([jnp.pad(w, pad) for w in (w_gate, w_up, w_down.T)], axis=1)
    block = exchange(jnp.broadcast_to(packed[None], (8, DROWS, 3 * HP)), False)
    first = block[:4].reshape(128, 3 * HP)
    second = block[4:].reshape(128, 3 * HP)
    a, p = [first], [second]
    b, m = [first], [second]
    for _ in range(3):
        a.append(ring(a[-1], 1))
        m.append(ring(m[-1], -1))
        p.append(ring(p[-1], 1))
        b.append(ring(b[-1], -1))
    a.append(ring(a[-1], 1))
    m.append(ring(m[-1], -1))

    own, k1, k2, k3, send, x_own, down = compute(
        inputs, gain, cotangent, (*a, *b[1:], *p, *m[1:])
    )

    arrived = exchange(down.reshape(8, 256, HP), True)
    (line,) = small_call(sum_kernel, [jax.ShapeDtypeStruct((256, HP), jnp.bfloat16)], arrived)
    quarter = jax.ShapeDtypeStruct((QUARTER, D), jnp.bfloat16)
    other = lax.ppermute(send, "c", [(0, 1), (1, 0)])
    own, *sums = small_call(
        pair_kernel,
        [jax.ShapeDtypeStruct((QUARTER, D), jnp.float32)] + [quarter] * 3,
        own, k1, k2, k3, other,
    )
    quarters = [along_x(s, k + 1) for k, s in enumerate(sums)]
    (mine,) = small_call(final_kernel, [quarter], x_own, gain.reshape(1, D), own, *quarters)
    mine, line = lax.optimization_barrier((mine, line))
    arrived = exchange(line.reshape(8, DROWS, HP), False)
    (total,) = small_call(sum_kernel, [jax.ShapeDtypeStruct((DROWS, HP), jnp.float32)], arrived)
    grad_down = total[:, :HU].T
    half = lax.all_gather(mine, "x", axis=0, tiled=True)
    away = lax.ppermute(half, "c", [(0, 1), (1, 0)])
    whole = jnp.zeros((TOK, D), jnp.bfloat16)
    whole = lax.dynamic_update_slice_in_dim(whole, half, c * HALF, 0)
    whole = lax.dynamic_update_slice_in_dim(whole, away, (1 - c) * HALF, 0)
    return whole, grad_down


def solution(mesh):
    split = Mesh(mesh.devices.reshape(NZ, NY, NX, NC), AXES)
    in_specs = (P(FS, None), P(), P(FS, TP), P(FS, TP), P(TP, FS), P(FS, None))
    out_specs = (P(FS, None), P(TP, FS))
    return jax.shard_map(
        shards, mesh=split, in_specs=in_specs, out_specs=out_specs, check_vma=False
    )
```

```python
import jax
import jax.numpy as jnp
from jax import lax
from jax.experimental import pallas as pl
from jax.experimental.pallas import tpu as pltpu
from jax.sharding import Mesh
from jax.sharding import PartitionSpec as P


AXES = ("z", "y", "x", "c")
NZ, NY, NX, NC = 8, 8, 4, 2
FS = ("z", "y")
TP = ("x", "c")
EPSILON = 1e-06
HALF_STEP = 0.5
TOK = 384
D = 2048
HU = 352
HP = 384
DROWS = 32
HALF = TOK // NC
QUARTER = HALF // NX
VMEM_LIMIT = 32 * 2**20
SMALL_LIMIT = 10 * 2**20


def device_number(z, y, x, c):
    return ((z % NZ * NY + y % NY) * NX + x) * NC + c


def ring_pairs(step):
    return [
        (device_number(z, y, x, c), device_number(z + (1 - c) * step, y + c * step, x, c))
        for z in range(NZ)
        for y in range(NY)
        for x in range(NX)
        for c in range(NC)
    ]


def line_groups(along_ring):
    groups = []
    for x in range(NX):
        for c in range(NC):
            vary_z = (c == 0) == along_ring
            for fixed in range(8):
                groups.append(
                    [
                        device_number(k, fixed, x, c) if vary_z else device_number(fixed, k, x, c)
                        for k in range(8)
                    ]
                )
    return groups


def ring(array, step):
    return lax.ppermute(array, AXES, ring_pairs(step))


def exchange(array, along_ring):
    return lax.all_to_all(
        array, AXES, 0, 0, axis_index_groups=line_groups(along_ring), tiled=True
    )


def dot(left, right, dims):
    return lax.dot_general(left, right, (dims, ((), ())), preferred_element_type=jnp.float32)


def compute_kernel(
    x_ref, gain_ref, cot_ref, b0, p1, p2, p3, p4, m1, m2, m3, m4,
    own_ref, k1_ref, k2_ref, k3_ref, send_ref, x_own_ref, down_ref, w_ref, xn_ref, dt_ref,
):
    x = lax.axis_index("x")
    c = lax.axis_index("c")
    r = jnp.where(c == 0, lax.axis_index("z"), lax.axis_index("y"))

    def row_of(q, o):
        q = lax.rem(q + 16, 8)
        return pl.multiple_of(jnp.where(c == 0, q * 256 + o * 32, o * 256 + q * 32), 32)

    def put(q, block, first, last):
        for o in range(first, last):
            w_ref[pl.ds(row_of(q, o), DROWS), :] = block[pl.ds((o - first) * DROWS, DROWS), :]

    put(r, b0, 0, 8)
    for k, block in enumerate((p1, p2, p3)):
        put(r - k - 1, block, 0, 8)
    for k, block in enumerate((m1, m2, m3)):
        put(r + k + 1, block, 0, 8)
    put(r + 4, p4, 0, 4)
    put(r + 4, m4, 4, 8)

    gain = gain_ref[...]
    for k in range(6):
        rows = pl.ds(k * 64, 64)
        value = x_ref[rows, :].astype(jnp.float32)
        inverse = lax.rsqrt(jnp.mean(value * value, axis=-1, keepdims=True) + EPSILON)
        xn_ref[rows, :] = (value * inverse * gain).astype(jnp.bfloat16)

    gate_up = dot(xn_ref[...], w_ref[:, : 2 * HP], ((1,), (0,)))
    gate = gate_up[:, :HP]
    up = gate_up[:, HP:]
    d_hidden = HALF_STEP * dot(cot_ref[...], w_ref[:, 2 * HP :], ((1,), (0,)))
    sig = jax.nn.sigmoid(gate)
    hidden = (gate * sig * up).astype(jnp.bfloat16)
    d_gate = (d_hidden * up * sig * (1.0 + gate * (1.0 - sig))).astype(jnp.bfloat16)
    d_up = (d_hidden * gate * sig).astype(jnp.bfloat16)
    both = jnp.concatenate([d_gate, d_up], axis=1)
    xn_ref[...] = dot(both, w_ref[:, : 2 * HP], ((1,), (1,))).astype(jnp.bfloat16)

    def quarter(core, k):
        row = core * HALF + lax.rem(x + k, NX) * QUARTER
        return pl.ds(pl.multiple_of(row, 16), QUARTER)

    for k, ref in enumerate((own_ref, k1_ref, k2_ref, k3_ref)):
        ref[...] = xn_ref[quarter(c, k), :]
        send_ref[pl.ds(k * QUARTER, QUARTER), :] = xn_ref[quarter(1 - c, k), :]
    x_own_ref[...] = x_ref[quarter(c, 0), :]
    dt_ref[...] = (HALF_STEP * dot(cot_ref[...], hidden, ((0,), (0,)))).astype(jnp.bfloat16)
    for q in range(8):
        for o in range(8):
            down_ref[pl.ds(q * 256 + o * 32, DROWS), :] = dt_ref[pl.ds(row_of(q, o), DROWS), :]


def vmem_specs(count):
    return [pl.BlockSpec(memory_space=pltpu.VMEM)] * count


def small_call(kernel, out_shape, *operands):
    count = len(out_shape)
    return pl.pallas_call(
        kernel,
        out_shape=tuple(out_shape),
        in_specs=vmem_specs(len(operands)),
        out_specs=tuple(vmem_specs(count)),
        compiler_params=pltpu.CompilerParams(vmem_limit_bytes=SMALL_LIMIT),
    )(*operands)


def compute(inputs, gain, cotangent, blocks):
    quarter = jax.ShapeDtypeStruct((QUARTER, D), jnp.bfloat16)
    return pl.pallas_call(
        compute_kernel,
        out_shape=(
            quarter, quarter, quarter, quarter,
            jax.ShapeDtypeStruct((HALF, D), jnp.bfloat16),
            quarter,
            jax.ShapeDtypeStruct((D, HP), jnp.bfloat16),
        ),
        in_specs=vmem_specs(3 + len(blocks)),
        out_specs=tuple(vmem_specs(7)),
        scratch_shapes=[
            pltpu.VMEM((D, 3 * HP), jnp.bfloat16),
            pltpu.VMEM((TOK, D), jnp.bfloat16),
            pltpu.VMEM((D, HP), jnp.bfloat16),
        ],
        compiler_params=pltpu.CompilerParams(vmem_limit_bytes=VMEM_LIMIT),
    )(inputs, gain.reshape(1, D), cotangent, *blocks)


def pair_kernel(own_ref, k1_ref, k2_ref, k3_ref, other_ref, s0_ref, s1_ref, s2_ref, s3_ref):
    kept = (own_ref, k1_ref, k2_ref, k3_ref)
    for k, out in enumerate((s0_ref, s1_ref, s2_ref, s3_ref)):
        other = other_ref[pl.ds(k * QUARTER, QUARTER), :].astype(jnp.float32)
        out[...] = (kept[k][...].astype(jnp.float32) + other).astype(out.dtype)


def final_kernel(x_ref, gain_ref, own_ref, q1_ref, q2_ref, q3_ref, out_ref):
    value = x_ref[...].astype(jnp.float32)
    inverse = lax.rsqrt(jnp.mean(value * value, axis=-1, keepdims=True) + EPSILON)
    normalized = value * inverse
    d_normed = own_ref[...]
    for ref in (q1_ref, q2_ref, q3_ref):
        d_normed = d_normed + ref[...].astype(jnp.float32)
    scaled = d_normed * gain_ref[...]
    mean = jnp.mean(scaled * normalized, axis=-1, keepdims=True)
    out_ref[...] = (inverse * (scaled - normalized * mean)).astype(jnp.bfloat16)


def sum_kernel(parts_ref, out_ref):
    total = parts_ref[0].astype(jnp.float32)
    for k in range(1, 8):
        total = total + parts_ref[k].astype(jnp.float32)
    out_ref[...] = total.astype(out_ref.dtype)


def along_x(array, step):
    return lax.ppermute(array, "x", [(k, (k + step) % NX) for k in range(NX)])


def shards(inputs, gain, w_gate, w_up, w_down, cotangent):
    c = lax.axis_index("c")
    pad = ((0, 0), (0, HP - HU))
    packed = jnp.concatenate([jnp.pad(w, pad) for w in (w_gate, w_up, w_down.T)], axis=1)
    block = exchange(jnp.broadcast_to(packed[None], (8, DROWS, 3 * HP)), False)
    b0 = block.reshape(256, 3 * HP)
    p2 = ring(b0, 2)
    m2 = ring(b0, -2)
    p1 = ring(b0, 1)
    m1 = ring(b0, -1)
    p3 = ring(p2, 1)
    m3 = ring(m2, -1)
    p4 = ring(p2[:128], 2)
    m4 = ring(m2[128:], -2)

    own, k1, k2, k3, send, x_own, down = compute(
        inputs, gain, cotangent, (b0, p1, p2, p3, p4, m1, m2, m3, m4)
    )

    arrived = exchange(down.reshape(8, 256, HP), True)
    (line,) = small_call(sum_kernel, [jax.ShapeDtypeStruct((256, HP), jnp.bfloat16)], arrived)
    quarter = jax.ShapeDtypeStruct((QUARTER, D), jnp.bfloat16)
    other = lax.ppermute(send, "c", [(0, 1), (1, 0)])
    own, *sums = small_call(
        pair_kernel,
        [jax.ShapeDtypeStruct((QUARTER, D), jnp.float32)] + [quarter] * 3,
        own, k1, k2, k3, other,
    )
    quarters = [along_x(s, k + 1) for k, s in enumerate(sums)]
    (mine,) = small_call(final_kernel, [quarter], x_own, gain.reshape(1, D), own, *quarters)
    mine, line = lax.optimization_barrier((mine, line))
    arrived = exchange(line.reshape(8, DROWS, HP), False)
    (total,) = small_call(sum_kernel, [jax.ShapeDtypeStruct((DROWS, HP), jnp.float32)], arrived)
    grad_down = total[:, :HU].T
    half = lax.all_gather(mine, "x", axis=0, tiled=True)
    away = lax.ppermute(half, "c", [(0, 1), (1, 0)])
    whole = jnp.zeros((TOK, D), jnp.bfloat16)
    whole = lax.dynamic_update_slice_in_dim(whole, half, c * HALF, 0)
    whole = lax.dynamic_update_slice_in_dim(whole, away, (1 - c) * HALF, 0)
    return whole, grad_down


def solution(mesh):
    split = Mesh(mesh.devices.reshape(NZ, NY, NX, NC), AXES)
    in_specs = (P(FS, None), P(), P(FS, TP), P(FS, TP), P(TP, FS), P(FS, None))
    out_specs = (P(FS, None), P(TP, FS))
    return jax.shard_map(
        shards, mesh=split, in_specs=in_specs, out_specs=out_specs, check_vma=False
    )
```

```python
import jax
import jax.numpy as jnp
from jax import lax
from jax.experimental import pallas as pl
from jax.experimental.pallas import tpu as pltpu
from jax.sharding import Mesh
from jax.sharding import PartitionSpec as P


AXES = ("z", "y", "x", "c")
NZ, NY, NX, NC = 8, 8, 4, 2
FS = ("z", "y")
TP = ("x", "c")
EPSILON = 1e-06
HALF_STEP = 0.5
TOK = 384
D = 2048
HU = 352
HP = 384
DROWS = 32
HALF = TOK // NC
QUARTER = HALF // NX
VMEM_LIMIT = 32 * 2**20
SMALL_LIMIT = 10 * 2**20
DOWN_LIMIT = 24 * 2**20


def device_number(z, y, x, c):
    return ((z % NZ * NY + y % NY) * NX + x) * NC + c


def ring_pairs(step):
    return [
        (device_number(z, y, x, c), device_number(z + (1 - c) * step, y + c * step, x, c))
        for z in range(NZ)
        for y in range(NY)
        for x in range(NX)
        for c in range(NC)
    ]


def line_groups(along_ring):
    groups = []
    for x in range(NX):
        for c in range(NC):
            vary_z = (c == 0) == along_ring
            for fixed in range(8):
                groups.append(
                    [
                        device_number(k, fixed, x, c) if vary_z else device_number(fixed, k, x, c)
                        for k in range(8)
                    ]
                )
    return groups


def ring(array, step):
    return lax.ppermute(array, AXES, ring_pairs(step))


def exchange(array, along_ring):
    return lax.all_to_all(
        array, AXES, 0, 0, axis_index_groups=line_groups(along_ring), tiled=True
    )


def dot(left, right, dims):
    return lax.dot_general(left, right, (dims, ((), ())), preferred_element_type=jnp.float32)


def partner(core, x, k):
    near = jnp.where(core == 0, 3 - x, x + 1 - 2 * lax.rem(x, 2))
    far = jnp.where(core == 0, x + 1 - 2 * lax.rem(x, 2), 3 - x)
    return (x, near, far, lax.rem(x + 2, NX))[k]


def quarter_rows(core, x, k):
    row = core * HALF + partner(core, x, k) * QUARTER
    return pl.ds(pl.multiple_of(row, 16), QUARTER)


def compute_kernel(
    x_ref, gain_ref, cot_ref, b0, p1, p2, p3, p4, m1, m2, m3, m4,
    keep_ref, send_ref, x_own_ref, hidden_ref, w_ref, xn_ref,
):
    x = lax.axis_index("x")
    c = lax.axis_index("c")
    r = jnp.where(c == 0, lax.axis_index("z"), lax.axis_index("y"))

    def row_of(q, o):
        q = lax.rem(q + 16, 8)
        return pl.multiple_of(jnp.where(c == 0, q * 256 + o * 32, o * 256 + q * 32), 32)

    def put(q, block, first, last):
        for o in range(first, last):
            w_ref[pl.ds(row_of(q, o), DROWS), :] = block[pl.ds((o - first) * DROWS, DROWS), :]

    put(r, b0, 0, 8)
    for k, block in enumerate((p1, p2, p3)):
        put(r - k - 1, block, 0, 8)
    for k, block in enumerate((m1, m2, m3)):
        put(r + k + 1, block, 0, 8)
    put(r + 4, p4, 0, 4)
    put(r + 4, m4, 4, 8)

    gain = gain_ref[...]
    for k in range(6):
        rows = pl.ds(k * 64, 64)
        value = x_ref[rows, :].astype(jnp.float32)
        inverse = lax.rsqrt(jnp.mean(value * value, axis=-1, keepdims=True) + EPSILON)
        xn_ref[rows, :] = (value * inverse * gain).astype(jnp.bfloat16)

    gate_up = dot(xn_ref[...], w_ref[:, : 2 * HP], ((1,), (0,)))
    gate = gate_up[:, :HP]
    up = gate_up[:, HP:]
    d_hidden = HALF_STEP * dot(cot_ref[...], w_ref[:, 2 * HP :], ((1,), (0,)))
    sig = jax.nn.sigmoid(gate)
    hidden = (gate * sig * up).astype(jnp.bfloat16)
    d_gate = (d_hidden * up * sig * (1.0 + gate * (1.0 - sig))).astype(jnp.bfloat16)
    d_up = (d_hidden * gate * sig).astype(jnp.bfloat16)
    both = jnp.concatenate([d_gate, d_up], axis=1)
    xn_ref[...] = dot(both, w_ref[:, : 2 * HP], ((1,), (1,))).astype(jnp.bfloat16)

    hidden_ref[...] = hidden
    for k in range(NX):
        rows = pl.ds(k * QUARTER, QUARTER)
        keep_ref[rows, :] = xn_ref[quarter_rows(c, x, k), :]
        send_ref[rows, :] = xn_ref[quarter_rows(1 - c, x, k), :]
    x_own_ref[...] = x_ref[quarter_rows(c, x, 0), :]


def down_kernel(cot_ref, hidden_ref, down_ref, dt_ref):
    c = lax.axis_index("c")
    dt = dot(cot_ref[...], hidden_ref[...], ((0,), (0,)))
    dt_ref[...] = (HALF_STEP * dt).astype(jnp.bfloat16)
    for q in range(8):
        for o in range(8):
            row = jnp.where(c == 0, q * 256 + o * 32, o * 256 + q * 32)
            rows = pl.ds(pl.multiple_of(row, 32), DROWS)
            down_ref[pl.ds(q * 256 + o * 32, DROWS), :] = dt_ref[rows, :]


def vmem_specs(count):
    return [pl.BlockSpec(memory_space=pltpu.VMEM)] * count


def small_call(kernel, out_shape, *operands):
    count = len(out_shape)
    return pl.pallas_call(
        kernel,
        out_shape=tuple(out_shape),
        in_specs=vmem_specs(len(operands)),
        out_specs=tuple(vmem_specs(count)),
        compiler_params=pltpu.CompilerParams(vmem_limit_bytes=SMALL_LIMIT),
    )(*operands)


def compute(inputs, gain, cotangent, blocks):
    half = jax.ShapeDtypeStruct((HALF, D), jnp.bfloat16)
    return pl.pallas_call(
        compute_kernel,
        out_shape=(
            half,
            half,
            jax.ShapeDtypeStruct((QUARTER, D), jnp.bfloat16),
            jax.ShapeDtypeStruct((TOK, HP), jnp.bfloat16),
        ),
        in_specs=vmem_specs(3 + len(blocks)),
        out_specs=tuple(vmem_specs(4)),
        scratch_shapes=[
            pltpu.VMEM((D, 3 * HP), jnp.bfloat16),
            pltpu.VMEM((TOK, D), jnp.bfloat16),
        ],
        compiler_params=pltpu.CompilerParams(vmem_limit_bytes=VMEM_LIMIT),
    )(inputs, gain, cotangent, *blocks)


def down_product(cotangent, hidden):
    return pl.pallas_call(
        down_kernel,
        out_shape=jax.ShapeDtypeStruct((D, HP), jnp.bfloat16),
        in_specs=vmem_specs(2),
        out_specs=vmem_specs(1)[0],
        scratch_shapes=[pltpu.VMEM((D, HP), jnp.bfloat16)],
        compiler_params=pltpu.CompilerParams(vmem_limit_bytes=DOWN_LIMIT),
    )(cotangent, hidden)


def pair_kernel(keep_ref, other_ref, sums_ref, out_ref):
    total = keep_ref[...].astype(jnp.float32) + other_ref[...].astype(jnp.float32)
    sums_ref[...] = total[: 2 * QUARTER]
    out_ref[...] = total[2 * QUARTER :].astype(jnp.bfloat16)


def second_kernel(sums_ref, got_ref, own_ref, out_ref):
    total = sums_ref[...] + got_ref[...].astype(jnp.float32)
    own_ref[...] = total[:QUARTER]
    out_ref[...] = total[QUARTER:].astype(jnp.bfloat16)


def final_kernel(x_ref, gain_ref, own_ref, got_ref, out_ref):
    value = x_ref[...].astype(jnp.float32)
    inverse = lax.rsqrt(jnp.mean(value * value, axis=-1, keepdims=True) + EPSILON)
    normalized = value * inverse
    scaled = (own_ref[...] + got_ref[...].astype(jnp.float32)) * gain_ref[...]
    mean = jnp.mean(scaled * normalized, axis=-1, keepdims=True)
    out_ref[...] = (inverse * (scaled - normalized * mean)).astype(jnp.bfloat16)


def join_kernel(first_ref, second_ref, out_ref):
    rows = first_ref.shape[0]
    out_ref[pl.ds(0, rows), :] = first_ref[...]
    out_ref[pl.ds(rows, rows), :] = second_ref[...]


def place_kernel(mine_ref, away_ref, out_ref, sems):
    x = lax.axis_index("x")
    c = lax.axis_index("c")
    copies = []
    for half, (core, ref) in enumerate(((c, mine_ref), (1 - c, away_ref))):
        for k in range(NX):
            copies.append(
                pltpu.make_async_copy(
                    ref.at[pl.ds(k * QUARTER, QUARTER), :],
                    out_ref.at[quarter_rows(core, x, k), :],
                    sems.at[half * NX + k],
                )
            )
    for copy in copies:
        copy.start()
    for copy in copies:
        copy.wait()


def place(mine, away):
    return pl.pallas_call(
        place_kernel,
        out_shape=jax.ShapeDtypeStruct((TOK, D), jnp.bfloat16),
        in_specs=vmem_specs(2),
        out_specs=pl.BlockSpec(memory_space=pl.ANY),
        scratch_shapes=[pltpu.SemaphoreType.DMA((2 * NX,))],
        compiler_params=pltpu.CompilerParams(vmem_limit_bytes=SMALL_LIMIT),
    )(mine, away)


def sum_kernel(parts_ref, out_ref):
    total = parts_ref[0].astype(jnp.float32)
    for k in range(1, 8):
        total = total + parts_ref[k].astype(jnp.float32)
    out_ref[...] = total.astype(out_ref.dtype)


def with_partner(array, first):
    pairs = [
        (device_number(z, y, x, c), device_number(z, y, x ^ (1 if (c == 0) == first else 3), c))
        for z in range(NZ)
        for y in range(NY)
        for x in range(NX)
        for c in range(NC)
    ]
    return lax.ppermute(array, AXES, pairs)


def with_core(array):
    return lax.ppermute(array, "c", [(0, 1), (1, 0)])


def shards(inputs, gain, w_gate, w_up, w_down, cotangent):
    pad = ((0, 0), (0, HP - HU))
    packed = jnp.concatenate([jnp.pad(w, pad) for w in (w_gate, w_up, w_down.T)], axis=1)
    block = exchange(jnp.broadcast_to(packed[None], (8, DROWS, 3 * HP)), False)
    b0 = block.reshape(256, 3 * HP)
    p2 = ring(b0, 2)
    m2 = ring(b0, -2)
    p1 = ring(b0, 1)
    m1 = ring(b0, -1)
    p3 = ring(p2, 1)
    m3 = ring(m2, -1)
    p4 = ring(p2[:128], 2)
    m4 = ring(m2[128:], -2)

    row = gain.reshape(1, D)
    keep, send, x_own, hidden = compute(
        inputs, row, cotangent, (b0, p1, p2, p3, p4, m1, m2, m3, m4)
    )
    other = with_core(send)
    down = down_product(cotangent, hidden)
    arrived = exchange(down.reshape(8, 256, HP), True)
    (line,) = small_call(sum_kernel, [jax.ShapeDtypeStruct((256, HP), jnp.bfloat16)], arrived)
    arrived = exchange(line.reshape(8, DROWS, HP), False)
    (total,) = small_call(sum_kernel, [jax.ShapeDtypeStruct((DROWS, HP), jnp.float32)], arrived)
    grad_down = total[:, :HU].T

    def shape(rows, kind=jnp.bfloat16):
        return jax.ShapeDtypeStruct((rows, D), kind)

    sums, out = small_call(
        pair_kernel, [shape(2 * QUARTER, jnp.float32), shape(2 * QUARTER)], keep, other
    )
    got = with_partner(out, True)
    own, out = small_call(second_kernel, [shape(QUARTER, jnp.float32), shape(QUARTER)], sums, got)
    got = with_partner(out, False)
    (mine,) = small_call(final_kernel, [shape(QUARTER)], x_own, row, own, got)
    got = with_partner(mine, False)
    (two,) = small_call(join_kernel, [shape(2 * QUARTER)], mine, got)
    got = with_partner(two, True)
    (four,) = small_call(join_kernel, [shape(HALF)], two, got)
    away = with_core(four)
    return place(four, away), grad_down


def solution(mesh):
    split = Mesh(mesh.devices.reshape(NZ, NY, NX, NC), AXES)
    in_specs = (P(FS, None), P(), P(FS, TP), P(FS, TP), P(TP, FS), P(FS, None))
    out_specs = (P(FS, None), P(TP, FS))
    return jax.shard_map(
        shards, mesh=split, in_specs=in_specs, out_specs=out_specs, check_vma=False
    )
```

```python
import jax
import jax.numpy as jnp
from jax import lax
from jax.experimental import pallas as pl
from jax.experimental.pallas import tpu as pltpu
from jax.sharding import Mesh
from jax.sharding import PartitionSpec as P


AXES = ("z", "y", "x", "c")
NZ, NY, NX, NC = 8, 8, 4, 2
FS = ("z", "y")
TP = ("x", "c")
EPSILON = 1e-06
HALF_STEP = 0.5
TOK = 384
D = 2048
HU = 352
HP = 384
DROWS = 32
HALF = TOK // NC
QUARTER = HALF // NX
VMEM_LIMIT = 28 * 2**20
SMALL_LIMIT = 6 * 2**20
DOWN_LIMIT = 16 * 2**20


def device_number(z, y, x, c):
    return ((z % NZ * NY + y % NY) * NX + x) * NC + c


def ring_pairs(step):
    return [
        (device_number(z, y, x, c), device_number(z + (1 - c) * step, y + c * step, x, c))
        for z in range(NZ)
        for y in range(NY)
        for x in range(NX)
        for c in range(NC)
    ]


def line_groups(along_ring):
    groups = []
    for x in range(NX):
        for c in range(NC):
            vary_z = (c == 0) == along_ring
            for fixed in range(8):
                groups.append(
                    [
                        device_number(k, fixed, x, c) if vary_z else device_number(fixed, k, x, c)
                        for k in range(8)
                    ]
                )
    return groups


def ring(array, step):
    return lax.ppermute(array, AXES, ring_pairs(step))


def exchange(array, along_ring):
    return lax.all_to_all(
        array, AXES, 0, 0, axis_index_groups=line_groups(along_ring), tiled=True
    )


def dot(left, right, dims):
    return lax.dot_general(left, right, (dims, ((), ())), preferred_element_type=jnp.float32)


def half_rows(core):
    return pl.ds(pl.multiple_of(core * HALF, 64), HALF)


def normalize_kernel(x_ref, gain_ref, xn_ref, half_ref):
    half_ref[...] = x_ref[half_rows(lax.axis_index("c")), :]
    gain = gain_ref[...]
    for k in range(6):
        rows = pl.ds(k * 64, 64)
        value = x_ref[rows, :].astype(jnp.float32)
        inverse = lax.rsqrt(jnp.mean(value * value, axis=-1, keepdims=True) + EPSILON)
        xn_ref[rows, :] = (value * inverse * gain).astype(jnp.bfloat16)


def compute_kernel(
    norm_ref, cot_ref, b0, p1, p2, p3, p4, m1, m2, m3, m4,
    keep_ref, send_ref, hidden_ref, w_ref, part_ref,
):
    c = lax.axis_index("c")
    r = jnp.where(c == 0, lax.axis_index("z"), lax.axis_index("y"))

    def row_of(q, o):
        q = lax.rem(q + 16, 8)
        return pl.multiple_of(jnp.where(c == 0, q * 256 + o * 32, o * 256 + q * 32), 32)

    def put(q, block, first, last):
        for o in range(first, last):
            w_ref[pl.ds(row_of(q, o), DROWS), :] = block[pl.ds((o - first) * DROWS, DROWS), :]

    put(r, b0, 0, 8)
    for k, block in enumerate((p1, p2, p3)):
        put(r - k - 1, block, 0, 8)
    for k, block in enumerate((m1, m2, m3)):
        put(r + k + 1, block, 0, 8)
    put(r + 4, p4, 0, 4)
    put(r + 4, m4, 4, 8)

    gate_up = dot(norm_ref[...], w_ref[:, : 2 * HP], ((1,), (0,)))
    gate = gate_up[:, :HP]
    up = gate_up[:, HP:]
    d_hidden = HALF_STEP * dot(cot_ref[...], w_ref[:, 2 * HP :], ((1,), (0,)))
    sig = jax.nn.sigmoid(gate)
    hidden = (gate * sig * up).astype(jnp.bfloat16)
    d_gate = (d_hidden * up * sig * (1.0 + gate * (1.0 - sig))).astype(jnp.bfloat16)
    d_up = (d_hidden * gate * sig).astype(jnp.bfloat16)
    both = jnp.concatenate([d_gate, d_up], axis=1)
    part_ref[...] = dot(both, w_ref[:, : 2 * HP], ((1,), (1,))).astype(jnp.bfloat16)
    hidden_ref[...] = hidden
    keep_ref[...] = part_ref[half_rows(c), :]
    send_ref[...] = part_ref[half_rows(1 - c), :]


def down_kernel(cot_ref, hidden_ref, down_ref, dt_ref, ordered_ref, sems):
    c = lax.axis_index("c")
    dt = dot(cot_ref[...], hidden_ref[...], ((0,), (0,)))
    dt_ref[...] = (HALF_STEP * dt).astype(jnp.bfloat16)
    copies = []
    for q in range(8):
        for o in range(8):
            row = jnp.where(c == 0, q * 256 + o * 32, o * 256 + q * 32)
            rows = pl.ds(pl.multiple_of(row, 32), DROWS)
            ordered_ref[pl.ds(q * 256 + o * 32, DROWS), :] = dt_ref[rows, :]
        block = pl.ds(q * 256, 256)
        copies.append(
            pltpu.make_async_copy(ordered_ref.at[block, :], down_ref.at[block, :], sems.at[q])
        )
        copies[-1].start()
    for copy in copies:
        copy.wait()


def vmem_specs(count):
    return [pl.BlockSpec(memory_space=pltpu.VMEM)] * count


def small_call(kernel, out_shape, *operands):
    count = len(out_shape)
    return pl.pallas_call(
        kernel,
        out_shape=tuple(out_shape),
        in_specs=vmem_specs(len(operands)),
        out_specs=tuple(vmem_specs(count)),
        compiler_params=pltpu.CompilerParams(vmem_limit_bytes=SMALL_LIMIT),
    )(*operands)


def compute(normed, cotangent, blocks):
    half = jax.ShapeDtypeStruct((HALF, D), jnp.bfloat16)
    return pl.pallas_call(
        compute_kernel,
        out_shape=(
            half,
            half,
            jax.ShapeDtypeStruct((TOK, HP), jnp.bfloat16),
        ),
        in_specs=vmem_specs(2 + len(blocks)),
        out_specs=tuple(vmem_specs(3)),
        scratch_shapes=[
            pltpu.VMEM((D, 3 * HP), jnp.bfloat16),
            pltpu.VMEM((TOK, D), jnp.bfloat16),
        ],
        compiler_params=pltpu.CompilerParams(vmem_limit_bytes=VMEM_LIMIT),
    )(normed, cotangent, *blocks)


def down_product(cotangent, hidden):
    return pl.pallas_call(
        down_kernel,
        out_shape=jax.ShapeDtypeStruct((D, HP), jnp.bfloat16),
        in_specs=vmem_specs(2),
        out_specs=pl.BlockSpec(memory_space=pltpu.HBM),
        scratch_shapes=[
            pltpu.VMEM((D, HP), jnp.bfloat16),
            pltpu.VMEM((D, HP), jnp.bfloat16),
            pltpu.SemaphoreType.DMA((8,)),
        ],
        compiler_params=pltpu.CompilerParams(vmem_limit_bytes=DOWN_LIMIT),
    )(cotangent, hidden)


def pair_kernel(left_ref, right_ref, out_ref):
    total = left_ref[...].astype(jnp.float32) + right_ref[...].astype(jnp.float32)
    out_ref[...] = total.astype(jnp.bfloat16)


def final_kernel(x_ref, gain_ref, left_ref, right_ref, out_ref):
    gain = gain_ref[...]
    for k in range(4):
        rows = pl.ds(k * QUARTER, QUARTER)
        value = x_ref[rows, :].astype(jnp.float32)
        inverse = lax.rsqrt(jnp.mean(value * value, axis=-1, keepdims=True) + EPSILON)
        normalized = value * inverse
        total = left_ref[rows, :].astype(jnp.float32) + right_ref[rows, :].astype(jnp.float32)
        scaled = total * gain
        mean = jnp.mean(scaled * normalized, axis=-1, keepdims=True)
        out_ref[rows, :] = (inverse * (scaled - normalized * mean)).astype(jnp.bfloat16)


def place_kernel(mine_ref, away_ref, out_ref, sems):
    c = lax.axis_index("c")
    copies = [
        pltpu.make_async_copy(ref, out_ref.at[half_rows(core), :], sems.at[k])
        for k, (core, ref) in enumerate(((c, mine_ref), (1 - c, away_ref)))
    ]
    for copy in copies:
        copy.start()
    for copy in copies:
        copy.wait()


def place(mine, away):
    return pl.pallas_call(
        place_kernel,
        out_shape=jax.ShapeDtypeStruct((TOK, D), jnp.bfloat16),
        in_specs=vmem_specs(2),
        out_specs=pl.BlockSpec(memory_space=pltpu.HBM),
        scratch_shapes=[pltpu.SemaphoreType.DMA((2,))],
        compiler_params=pltpu.CompilerParams(vmem_limit_bytes=SMALL_LIMIT),
    )(mine, away)


def sum_kernel(parts_ref, out_ref):
    total = parts_ref[0].astype(jnp.float32)
    for k in range(1, 8):
        total = total + parts_ref[k].astype(jnp.float32)
    out_ref[...] = total.astype(out_ref.dtype)


def with_partner(array, first):
    pairs = [
        (device_number(z, y, x, c), device_number(z, y, x ^ (1 if (c == 0) == first else 3), c))
        for z in range(NZ)
        for y in range(NY)
        for x in range(NX)
        for c in range(NC)
    ]
    return lax.ppermute(array, AXES, pairs)


def with_core(array):
    return lax.ppermute(array, "c", [(0, 1), (1, 0)])


def shards(inputs, gain, w_gate, w_up, w_down, cotangent):
    pad = ((0, 0), (0, HP - HU))
    packed = jnp.concatenate([jnp.pad(w, pad) for w in (w_gate, w_up, w_down.T)], axis=1)
    block = exchange(jnp.broadcast_to(packed[None], (8, DROWS, 3 * HP)), False)
    b0 = block.reshape(256, 3 * HP)
    p2 = ring(b0, 2)
    m2 = ring(b0, -2)
    p1 = ring(b0, 1)
    m1 = ring(b0, -1)
    p3 = ring(p2, 1)
    m3 = ring(m2, -1)
    p4 = ring(p2[:128], 2)
    m4 = ring(m2[128:], -2)

    row = gain.reshape(1, D)
    half = jax.ShapeDtypeStruct((HALF, D), jnp.bfloat16)
    normed, x_half = small_call(
        normalize_kernel, [jax.ShapeDtypeStruct((TOK, D), jnp.bfloat16), half], inputs, row
    )
    keep, send, hidden = compute(normed, cotangent, (b0, p1, p2, p3, p4, m1, m2, m3, m4))
    other = with_core(send)
    down = down_product(cotangent, hidden)
    arrived = exchange(down.reshape(8, 256, HP), True)
    (line,) = small_call(sum_kernel, [jax.ShapeDtypeStruct((256, HP), jnp.bfloat16)], arrived)
    arrived = exchange(line.reshape(8, DROWS, HP), False)
    (total,) = small_call(sum_kernel, [jax.ShapeDtypeStruct((DROWS, HP), jnp.float32)], arrived)
    grad_down = total[:, :HU].T

    (chip,) = small_call(pair_kernel, [half], keep, other)
    got = with_partner(chip, True)
    (two,) = small_call(pair_kernel, [half], chip, got)
    got = with_partner(two, False)
    (mine,) = small_call(final_kernel, [half], x_half, row, two, got)
    away = with_core(mine)
    return place(mine, away), grad_down


def solution(mesh):
    split = Mesh(mesh.devices.reshape(NZ, NY, NX, NC), AXES)
    in_specs = (P(FS, None), P(), P(FS, TP), P(FS, TP), P(TP, FS), P(FS, None))
    out_specs = (P(FS, None), P(TP, FS))
    return jax.shard_map(
        shards, mesh=split, in_specs=in_specs, out_specs=out_specs, check_vma=False
    )
```

```python
import jax
import jax.numpy as jnp
from jax import lax
from jax.experimental import pallas as pl
from jax.experimental.pallas import tpu as pltpu
from jax.sharding import Mesh
from jax.sharding import PartitionSpec as P


AXES = ("z", "y", "x", "c")
NZ, NY, NX, NC = 8, 8, 4, 2
FS = ("z", "y")
TP = ("x", "c")
EPSILON = 1e-06
HALF_STEP = 0.5
TOK = 384
D = 2048
HU = 352
HP = 384
DROWS = 32
HALF = TOK // NC
QUARTER = HALF // NX
VMEM_LIMIT = 28 * 2**20
SMALL_LIMIT = 6 * 2**20
DOWN_LIMIT = 16 * 2**20


def device_number(z, y, x, c):
    return ((z % NZ * NY + y % NY) * NX + x) * NC + c


def ring_pairs(step):
    return [
        (device_number(z, y, x, c), device_number(z + (1 - c) * step, y + c * step, x, c))
        for z in range(NZ)
        for y in range(NY)
        for x in range(NX)
        for c in range(NC)
    ]


def line_groups(along_ring):
    groups = []
    for x in range(NX):
        for c in range(NC):
            vary_z = (c == 0) == along_ring
            for fixed in range(8):
                groups.append(
                    [
                        device_number(k, fixed, x, c) if vary_z else device_number(fixed, k, x, c)
                        for k in range(8)
                    ]
                )
    return groups


def ring(array, step):
    return lax.ppermute(array, AXES, ring_pairs(step))


def exchange(array, along_ring):
    return lax.all_to_all(
        array, AXES, 0, 0, axis_index_groups=line_groups(along_ring), tiled=True
    )


def dot(left, right, dims):
    return lax.dot_general(left, right, (dims, ((), ())), preferred_element_type=jnp.float32)


def half_rows(core):
    return pl.ds(pl.multiple_of(core * HALF, 64), HALF)


def normalize_kernel(x_ref, gain_ref, xn_ref, half_ref):
    half_ref[...] = x_ref[half_rows(lax.axis_index("c")), :]
    gain = gain_ref[...]
    for k in range(6):
        rows = pl.ds(k * 64, 64)
        value = x_ref[rows, :].astype(jnp.float32)
        inverse = lax.rsqrt(jnp.mean(value * value, axis=-1, keepdims=True) + EPSILON)
        xn_ref[rows, :] = (value * inverse * gain).astype(jnp.bfloat16)


def compute_kernel(
    norm_ref, cot_ref, b0, p1, p2, p3, p4, m1, m2, m3, m4,
    keep_ref, send_ref, hidden_ref, w_ref, part_ref,
):
    c = lax.axis_index("c")
    r = jnp.where(c == 0, lax.axis_index("z"), lax.axis_index("y"))

    def row_of(q, o):
        q = lax.rem(q + 16, 8)
        return pl.multiple_of(jnp.where(c == 0, q * 256 + o * 32, o * 256 + q * 32), 32)

    def put(q, block, first, last):
        for o in range(first, last):
            w_ref[pl.ds(row_of(q, o), DROWS), :] = block[pl.ds((o - first) * DROWS, DROWS), :]

    put(r, b0, 0, 8)
    for k, block in enumerate((p1, p2, p3)):
        put(r - k - 1, block, 0, 8)
    for k, block in enumerate((m1, m2, m3)):
        put(r + k + 1, block, 0, 8)
    put(r + 4, p4, 0, 4)
    put(r + 4, m4, 4, 8)

    gate_up = dot(norm_ref[...], w_ref[:, : 2 * HP], ((1,), (0,)))
    gate = gate_up[:, :HP]
    up = gate_up[:, HP:]
    d_hidden = HALF_STEP * dot(cot_ref[...], w_ref[:, 2 * HP :], ((1,), (0,)))
    sig = jax.nn.sigmoid(gate)
    hidden = (gate * sig * up).astype(jnp.bfloat16)
    d_gate = (d_hidden * up * sig * (1.0 + gate * (1.0 - sig))).astype(jnp.bfloat16)
    d_up = (d_hidden * gate * sig).astype(jnp.bfloat16)
    both = jnp.concatenate([d_gate, d_up], axis=1)
    part_ref[...] = dot(both, w_ref[:, : 2 * HP], ((1,), (1,))).astype(jnp.bfloat16)
    hidden_ref[...] = hidden
    keep_ref[...] = part_ref[half_rows(c), :]
    send_ref[...] = part_ref[half_rows(1 - c), :]


def down_kernel(cot_ref, hidden_ref, down_ref, dt_ref, ordered_ref, sems):
    c = lax.axis_index("c")
    dt = dot(cot_ref[...], hidden_ref[...], ((0,), (0,)))
    dt_ref[...] = (HALF_STEP * dt).astype(jnp.bfloat16)
    copies = []
    for q in range(8):
        for o in range(8):
            row = jnp.where(c == 0, q * 256 + o * 32, o * 256 + q * 32)
            rows = pl.ds(pl.multiple_of(row, 32), DROWS)
            ordered_ref[pl.ds(q * 256 + o * 32, DROWS), :] = dt_ref[rows, :]
        block = pl.ds(q * 256, 256)
        copies.append(
            pltpu.make_async_copy(ordered_ref.at[block, :], down_ref.at[block, :], sems.at[q])
        )
        copies[-1].start()
    for copy in copies:
        copy.wait()


def vmem_specs(count):
    return [pl.BlockSpec(memory_space=pltpu.VMEM)] * count


def small_call(kernel, out_shape, *operands):
    count = len(out_shape)
    return pl.pallas_call(
        kernel,
        out_shape=tuple(out_shape),
        in_specs=vmem_specs(len(operands)),
        out_specs=tuple(vmem_specs(count)),
        compiler_params=pltpu.CompilerParams(vmem_limit_bytes=SMALL_LIMIT),
    )(*operands)


def compute(normed, cotangent, blocks):
    half = jax.ShapeDtypeStruct((HALF, D), jnp.bfloat16)
    return pl.pallas_call(
        compute_kernel,
        out_shape=(
            half,
            half,
            jax.ShapeDtypeStruct((TOK, HP), jnp.bfloat16),
        ),
        in_specs=vmem_specs(2 + len(blocks)),
        out_specs=tuple(vmem_specs(3)),
        scratch_shapes=[
            pltpu.VMEM((D, 3 * HP), jnp.bfloat16),
            pltpu.VMEM((TOK, D), jnp.bfloat16),
        ],
        compiler_params=pltpu.CompilerParams(vmem_limit_bytes=VMEM_LIMIT),
    )(normed, cotangent, *blocks)


def down_product(cotangent, hidden):
    return pl.pallas_call(
        down_kernel,
        out_shape=jax.ShapeDtypeStruct((D, HP), jnp.bfloat16),
        in_specs=vmem_specs(2),
        out_specs=pl.BlockSpec(memory_space=pltpu.HBM),
        scratch_shapes=[
            pltpu.VMEM((D, HP), jnp.bfloat16),
            pltpu.VMEM((D, HP), jnp.bfloat16),
            pltpu.SemaphoreType.DMA((8,)),
        ],
        compiler_params=pltpu.CompilerParams(vmem_limit_bytes=DOWN_LIMIT),
    )(cotangent, hidden)


def pair_kernel(left_ref, right_ref, *out_refs):
    total = left_ref[...].astype(jnp.float32) + right_ref[...].astype(jnp.float32)
    rows = total.shape[0] // len(out_refs)
    for k, out in enumerate(out_refs):
        out[...] = total[k * rows : (k + 1) * rows].astype(jnp.bfloat16)


def final_kernel(x_ref, gain_ref, left1, right1, left2, right2, out_ref):
    gain = gain_ref[...]
    for k in range(4):
        rows = pl.ds(k * QUARTER, QUARTER)
        part = pl.ds(k % 2 * QUARTER, QUARTER)
        left, right = ((left1, right1), (left2, right2))[k // 2]
        value = x_ref[rows, :].astype(jnp.float32)
        inverse = lax.rsqrt(jnp.mean(value * value, axis=-1, keepdims=True) + EPSILON)
        normalized = value * inverse
        total = left[part, :].astype(jnp.float32) + right[part, :].astype(jnp.float32)
        scaled = total * gain
        mean = jnp.mean(scaled * normalized, axis=-1, keepdims=True)
        out_ref[rows, :] = (inverse * (scaled - normalized * mean)).astype(jnp.bfloat16)


def place_kernel(mine_ref, away_ref, out_ref, sems):
    c = lax.axis_index("c")
    copies = [
        pltpu.make_async_copy(ref, out_ref.at[half_rows(core), :], sems.at[k])
        for k, (core, ref) in enumerate(((c, mine_ref), (1 - c, away_ref)))
    ]
    for copy in copies:
        copy.start()
    for copy in copies:
        copy.wait()


def place(mine, away):
    return pl.pallas_call(
        place_kernel,
        out_shape=jax.ShapeDtypeStruct((TOK, D), jnp.bfloat16),
        in_specs=vmem_specs(2),
        out_specs=pl.BlockSpec(memory_space=pltpu.HBM),
        scratch_shapes=[pltpu.SemaphoreType.DMA((2,))],
        compiler_params=pltpu.CompilerParams(vmem_limit_bytes=SMALL_LIMIT),
    )(mine, away)


def sum_kernel(parts_ref, out_ref):
    total = parts_ref[0].astype(jnp.float32)
    for k in range(1, 8):
        total = total + parts_ref[k].astype(jnp.float32)
    out_ref[...] = total.astype(out_ref.dtype)


def with_partner(array, first):
    pairs = [
        (device_number(z, y, x, c), device_number(z, y, x ^ (1 if (c == 0) == first else 3), c))
        for z in range(NZ)
        for y in range(NY)
        for x in range(NX)
        for c in range(NC)
    ]
    return lax.ppermute(array, AXES, pairs)


def with_core(array):
    return lax.ppermute(array, "c", [(0, 1), (1, 0)])


def shards(inputs, gain, w_gate, w_up, w_down, cotangent):
    pad = ((0, 0), (0, HP - HU))
    packed = jnp.concatenate([jnp.pad(w, pad) for w in (w_gate, w_up, w_down.T)], axis=1)
    block = exchange(jnp.broadcast_to(packed[None], (8, DROWS, 3 * HP)), False)
    b0 = block.reshape(256, 3 * HP)
    p2 = ring(b0, 2)
    m2 = ring(b0, -2)
    p1 = ring(b0, 1)
    m1 = ring(b0, -1)
    p3 = ring(p2, 1)
    m3 = ring(m2, -1)
    p4 = ring(p2[:128], 2)
    m4 = ring(m2[128:], -2)

    row = gain.reshape(1, D)
    half = jax.ShapeDtypeStruct((HALF, D), jnp.bfloat16)
    normed, x_half = small_call(
        normalize_kernel, [jax.ShapeDtypeStruct((TOK, D), jnp.bfloat16), half], inputs, row
    )
    keep, send, hidden = compute(normed, cotangent, (b0, p1, p2, p3, p4, m1, m2, m3, m4))
    other = with_core(send)
    down = down_product(cotangent, hidden)
    arrived = exchange(down.reshape(8, 256, HP), True)
    (line,) = small_call(sum_kernel, [jax.ShapeDtypeStruct((256, HP), jnp.bfloat16)], arrived)
    arrived = exchange(line.reshape(8, DROWS, HP), False)
    (total,) = small_call(sum_kernel, [jax.ShapeDtypeStruct((DROWS, HP), jnp.float32)], arrived)
    grad_down = total[:, :HU].T

    piece = jax.ShapeDtypeStruct((HALF // 2, D), jnp.bfloat16)
    chip1, chip2 = small_call(pair_kernel, [piece, piece], keep, other)
    got1 = with_partner(chip1, True)
    got2 = with_partner(chip2, True)
    (two1,) = small_call(pair_kernel, [piece], chip1, got1)
    far1 = with_partner(two1, False)
    (two2,) = small_call(pair_kernel, [piece], chip2, got2)
    far2 = with_partner(two2, False)
    (mine,) = small_call(final_kernel, [half], x_half, row, two1, far1, two2, far2)
    away = with_core(mine)
    return place(mine, away), grad_down


def solution(mesh):
    split = Mesh(mesh.devices.reshape(NZ, NY, NX, NC), AXES)
    in_specs = (P(FS, None), P(), P(FS, TP), P(FS, TP), P(TP, FS), P(FS, None))
    out_specs = (P(FS, None), P(TP, FS))
    return jax.shard_map(
        shards, mesh=split, in_specs=in_specs, out_specs=out_specs, check_vma=False
    )
```

```python
import jax
import jax.numpy as jnp
from jax import lax
from jax.experimental import pallas as pl
from jax.experimental.pallas import tpu as pltpu
from jax.sharding import Mesh
from jax.sharding import PartitionSpec as P


AXES = ("z", "y", "x", "c")
NZ, NY, NX, NC = 8, 8, 4, 2
FS = ("z", "y")
TP = ("x", "c")
EPSILON = 1e-06
HALF_STEP = 0.5
TOK = 384
D = 2048
HU = 352
HP = 384
DROWS = 32
HALF = TOK // NC
QUARTER = HALF // NX
VMEM_LIMIT = 28 * 2**20
SMALL_LIMIT = 6 * 2**20
DOWN_LIMIT = 16 * 2**20


def device_number(z, y, x, c):
    return ((z % NZ * NY + y % NY) * NX + x) * NC + c


def ring_pairs(step):
    return [
        (device_number(z, y, x, c), device_number(z + (1 - c) * step, y + c * step, x, c))
        for z in range(NZ)
        for y in range(NY)
        for x in range(NX)
        for c in range(NC)
    ]


def line_groups(along_ring):
    groups = []
    for x in range(NX):
        for c in range(NC):
            vary_z = (c == 0) == along_ring
            for fixed in range(8):
                groups.append(
                    [
                        device_number(k, fixed, x, c) if vary_z else device_number(fixed, k, x, c)
                        for k in range(8)
                    ]
                )
    return groups


def ring(array, step):
    return lax.ppermute(array, AXES, ring_pairs(step))


def exchange(array, along_ring):
    return lax.all_to_all(
        array, AXES, 0, 0, axis_index_groups=line_groups(along_ring), tiled=True
    )


def dot(left, right, dims):
    return lax.dot_general(left, right, (dims, ((), ())), preferred_element_type=jnp.float32)


def half_rows(core):
    return pl.ds(pl.multiple_of(core * HALF, 64), HALF)


def normalize_kernel(x_ref, gain_ref, xn_ref, half_ref):
    half_ref[...] = x_ref[half_rows(lax.axis_index("c")), :]
    gain = gain_ref[...]
    for k in range(6):
        rows = pl.ds(k * 64, 64)
        value = x_ref[rows, :].astype(jnp.float32)
        inverse = lax.rsqrt(jnp.mean(value * value, axis=-1, keepdims=True) + EPSILON)
        xn_ref[rows, :] = (value * inverse * gain).astype(jnp.bfloat16)


def compute_kernel(
    norm_ref, cot_ref, b0, p1, p2, p3, p4, m1, m2, m3, m4,
    keep_ref, send_ref, hidden_ref, w_ref, part_ref,
):
    c = lax.axis_index("c")
    r = jnp.where(c == 0, lax.axis_index("z"), lax.axis_index("y"))

    def row_of(q, o):
        q = lax.rem(q + 16, 8)
        return pl.multiple_of(jnp.where(c == 0, q * 256 + o * 32, o * 256 + q * 32), 32)

    def put(q, block, first, last):
        for o in range(first, last):
            w_ref[pl.ds(row_of(q, o), DROWS), :] = block[pl.ds((o - first) * DROWS, DROWS), :]

    put(r, b0, 0, 8)
    for k, block in enumerate((p1, p2, p3)):
        put(r - k - 1, block, 0, 8)
    for k, block in enumerate((m1, m2, m3)):
        put(r + k + 1, block, 0, 8)
    put(r + 4, p4, 0, 4)
    put(r + 4, m4, 4, 8)

    gate_up = dot(norm_ref[...], w_ref[:, : 2 * HP], ((1,), (0,)))
    gate = gate_up[:, :HP]
    up = gate_up[:, HP:]
    d_hidden = HALF_STEP * dot(cot_ref[...], w_ref[:, 2 * HP :], ((1,), (0,)))
    sig = jax.nn.sigmoid(gate)
    hidden = (gate * sig * up).astype(jnp.bfloat16)
    d_gate = (d_hidden * up * sig * (1.0 + gate * (1.0 - sig))).astype(jnp.bfloat16)
    d_up = (d_hidden * gate * sig).astype(jnp.bfloat16)
    both = jnp.concatenate([d_gate, d_up], axis=1)
    part_ref[...] = dot(both, w_ref[:, : 2 * HP], ((1,), (1,))).astype(jnp.bfloat16)
    hidden_ref[...] = hidden
    keep_ref[...] = part_ref[half_rows(c), :]
    send_ref[...] = part_ref[half_rows(1 - c), :]


def turn_kernel(cot_ref, turned_ref):
    c = lax.axis_index("c")
    for z in range(NZ):
        block = cot_ref[:, z * 256 : (z + 1) * 256].T
        for y in range(NY):
            row = jnp.where(c == 0, z * 256 + y * 32, y * 256 + z * 32)
            rows = pl.ds(pl.multiple_of(row, 32), DROWS)
            turned_ref[rows, :] = block[y * 32 : (y + 1) * 32, :]


def down_kernel(turned_ref, hidden_ref, down_ref):
    down = HALF_STEP * dot(turned_ref[...], hidden_ref[...], ((1,), (0,)))
    down_ref[...] = down.astype(jnp.bfloat16)


def vmem_specs(count):
    return [pl.BlockSpec(memory_space=pltpu.VMEM)] * count


def small_call(kernel, out_shape, *operands):
    count = len(out_shape)
    return pl.pallas_call(
        kernel,
        out_shape=tuple(out_shape),
        in_specs=vmem_specs(len(operands)),
        out_specs=tuple(vmem_specs(count)),
        compiler_params=pltpu.CompilerParams(vmem_limit_bytes=SMALL_LIMIT),
    )(*operands)


def compute(normed, cotangent, blocks):
    half = jax.ShapeDtypeStruct((HALF, D), jnp.bfloat16)
    return pl.pallas_call(
        compute_kernel,
        out_shape=(
            half,
            half,
            jax.ShapeDtypeStruct((TOK, HP), jnp.bfloat16),
        ),
        in_specs=vmem_specs(2 + len(blocks)),
        out_specs=tuple(vmem_specs(3)),
        scratch_shapes=[
            pltpu.VMEM((D, 3 * HP), jnp.bfloat16),
            pltpu.VMEM((TOK, D), jnp.bfloat16),
        ],
        compiler_params=pltpu.CompilerParams(vmem_limit_bytes=VMEM_LIMIT),
    )(normed, cotangent, *blocks)


def one_call(kernel, out_shape, *operands):
    return pl.pallas_call(
        kernel,
        out_shape=out_shape,
        in_specs=vmem_specs(len(operands)),
        out_specs=vmem_specs(1)[0],
        compiler_params=pltpu.CompilerParams(vmem_limit_bytes=DOWN_LIMIT),
    )(*operands)


def pair_kernel(left_ref, right_ref, *out_refs):
    total = left_ref[...].astype(jnp.float32) + right_ref[...].astype(jnp.float32)
    rows = total.shape[0] // len(out_refs)
    for k, out in enumerate(out_refs):
        out[...] = total[k * rows : (k + 1) * rows].astype(jnp.bfloat16)


def final_kernel(x_ref, gain_ref, left1, right1, left2, right2, out_ref):
    gain = gain_ref[...]
    for k in range(4):
        rows = pl.ds(k * QUARTER, QUARTER)
        part = pl.ds(k % 2 * QUARTER, QUARTER)
        left, right = ((left1, right1), (left2, right2))[k // 2]
        value = x_ref[rows, :].astype(jnp.float32)
        inverse = lax.rsqrt(jnp.mean(value * value, axis=-1, keepdims=True) + EPSILON)
        normalized = value * inverse
        total = left[part, :].astype(jnp.float32) + right[part, :].astype(jnp.float32)
        scaled = total * gain
        mean = jnp.mean(scaled * normalized, axis=-1, keepdims=True)
        out_ref[rows, :] = (inverse * (scaled - normalized * mean)).astype(jnp.bfloat16)


def place_kernel(mine_ref, away_ref, out_ref, sems):
    c = lax.axis_index("c")
    copies = [
        pltpu.make_async_copy(ref, out_ref.at[half_rows(core), :], sems.at[k])
        for k, (core, ref) in enumerate(((c, mine_ref), (1 - c, away_ref)))
    ]
    for copy in copies:
        copy.start()
    for copy in copies:
        copy.wait()


def place(mine, away):
    return pl.pallas_call(
        place_kernel,
        out_shape=jax.ShapeDtypeStruct((TOK, D), jnp.bfloat16),
        in_specs=vmem_specs(2),
        out_specs=pl.BlockSpec(memory_space=pltpu.HBM),
        scratch_shapes=[pltpu.SemaphoreType.DMA((2,))],
        compiler_params=pltpu.CompilerParams(vmem_limit_bytes=SMALL_LIMIT),
    )(mine, away)


def sum_kernel(parts_ref, out_ref):
    total = parts_ref[0].astype(jnp.float32)
    for k in range(1, 8):
        total = total + parts_ref[k].astype(jnp.float32)
    out_ref[...] = total[:, : out_ref.shape[1]].astype(out_ref.dtype)


def with_partner(array, first):
    pairs = [
        (device_number(z, y, x, c), device_number(z, y, x ^ (1 if (c == 0) == first else 3), c))
        for z in range(NZ)
        for y in range(NY)
        for x in range(NX)
        for c in range(NC)
    ]
    return lax.ppermute(array, AXES, pairs)


def with_core(array):
    return lax.ppermute(array, "c", [(0, 1), (1, 0)])


def shards(inputs, gain, w_gate, w_up, w_down, cotangent):
    pad = ((0, 0), (0, HP - HU))
    packed = jnp.concatenate([jnp.pad(w, pad) for w in (w_gate, w_up, w_down.T)], axis=1)
    block = exchange(jnp.broadcast_to(packed[None], (8, DROWS, 3 * HP)), False)
    b0 = block.reshape(256, 3 * HP)
    p2 = ring(b0, 2)
    m2 = ring(b0, -2)
    p1 = ring(b0, 1)
    m1 = ring(b0, -1)
    p3 = ring(p2, 1)
    m3 = ring(m2, -1)
    p4 = ring(p2[:128], 2)
    m4 = ring(m2[128:], -2)

    row = gain.reshape(1, D)
    half = jax.ShapeDtypeStruct((HALF, D), jnp.bfloat16)
    normed, x_half = small_call(
        normalize_kernel, [jax.ShapeDtypeStruct((TOK, D), jnp.bfloat16), half], inputs, row
    )
    turned = one_call(turn_kernel, jax.ShapeDtypeStruct((D, TOK), jnp.bfloat16), cotangent)
    keep, send, hidden = compute(normed, cotangent, (b0, p1, p2, p3, p4, m1, m2, m3, m4))
    other = with_core(send)
    down = one_call(
        down_kernel, jax.ShapeDtypeStruct((D, HP), jnp.bfloat16), turned, hidden
    )
    arrived = exchange(down.reshape(8, 256, HP), True)
    (line,) = small_call(sum_kernel, [jax.ShapeDtypeStruct((256, HP), jnp.bfloat16)], arrived)
    arrived = exchange(line.reshape(8, DROWS, HP), False)
    (total,) = small_call(sum_kernel, [jax.ShapeDtypeStruct((DROWS, HU), jnp.float32)], arrived)
    grad_down = total.T

    piece = jax.ShapeDtypeStruct((HALF // 2, D), jnp.bfloat16)
    chip1, chip2 = small_call(pair_kernel, [piece, piece], keep, other)
    got1 = with_partner(chip1, True)
    got2 = with_partner(chip2, True)
    (two1,) = small_call(pair_kernel, [piece], chip1, got1)
    far1 = with_partner(two1, False)
    (two2,) = small_call(pair_kernel, [piece], chip2, got2)
    far2 = with_partner(two2, False)
    (mine,) = small_call(final_kernel, [half], x_half, row, two1, far1, two2, far2)
    away = with_core(mine)
    whole = place(mine, away)
    return whole, grad_down


def solution(mesh):
    split = Mesh(mesh.devices.reshape(NZ, NY, NX, NC), AXES)
    in_specs = (P(FS, None), P(), P(FS, TP), P(FS, TP), P(TP, FS), P(FS, None))
    out_specs = (P(FS, None), P(TP, FS))
    return jax.shard_map(
        shards, mesh=split, in_specs=in_specs, out_specs=out_specs, check_vma=False
    )
```

```python
import jax
import jax.numpy as jnp
from jax import lax
from jax.experimental import pallas as pl
from jax.experimental.pallas import tpu as pltpu
from jax.sharding import Mesh
from jax.sharding import PartitionSpec as P


AXES = ("z", "y", "x", "c")
NZ, NY, NX, NC = 8, 8, 4, 2
FS = ("z", "y")
TP = ("x", "c")
EPSILON = 1e-06
HALF_STEP = 0.5
TOK = 384
D = 2048
HU = 352
HP = 384
DROWS = 32
HALF = TOK // NC
QUARTER = HALF // NX
VMEM_LIMIT = 28 * 2**20
SMALL_LIMIT = 6 * 2**20
DOWN_LIMIT = 16 * 2**20


def device_number(z, y, x, c):
    return ((z % NZ * NY + y % NY) * NX + x) * NC + c


def ring_pairs(step):
    return [
        (device_number(z, y, x, c), device_number(z + (1 - c) * step, y + c * step, x, c))
        for z in range(NZ)
        for y in range(NY)
        for x in range(NX)
        for c in range(NC)
    ]


def line_groups(along_ring):
    groups = []
    for x in range(NX):
        for c in range(NC):
            vary_z = (c == 0) == along_ring
            for fixed in range(8):
                groups.append(
                    [
                        device_number(k, fixed, x, c) if vary_z else device_number(fixed, k, x, c)
                        for k in range(8)
                    ]
                )
    return groups


def ring(array, step):
    return lax.ppermute(array, AXES, ring_pairs(step))


def exchange(array, along_ring):
    return lax.all_to_all(
        array, AXES, 0, 0, axis_index_groups=line_groups(along_ring), tiled=True
    )


def dot(left, right, dims):
    return lax.dot_general(left, right, (dims, ((), ())), preferred_element_type=jnp.float32)


def half_rows(core):
    return pl.ds(pl.multiple_of(core * HALF, 64), HALF)


def normalize_kernel(x_ref, gain_ref, xn_ref, half_ref):
    half_ref[...] = x_ref[half_rows(lax.axis_index("c")), :]
    gain = gain_ref[...]
    for k in range(6):
        rows = pl.ds(k * 64, 64)
        value = x_ref[rows, :].astype(jnp.float32)
        inverse = lax.rsqrt(jnp.mean(value * value, axis=-1, keepdims=True) + EPSILON)
        xn_ref[rows, :] = (value * inverse * gain).astype(jnp.bfloat16)


def compute_kernel(
    norm_ref, cot_ref, b0, p1, p2, p3, p4, m1, m2, m3, m4,
    keep_ref, send_ref, hidden_ref, w_ref, part_ref,
):
    c = lax.axis_index("c")
    r = jnp.where(c == 0, lax.axis_index("z"), lax.axis_index("y"))

    def row_of(q, o):
        q = lax.rem(q + 16, 8)
        return pl.multiple_of(jnp.where(c == 0, q * 256 + o * 32, o * 256 + q * 32), 32)

    def put(q, block, first, last):
        for o in range(first, last):
            w_ref[pl.ds(row_of(q, o), DROWS), :] = block[pl.ds((o - first) * DROWS, DROWS), :]

    put(r, b0, 0, 8)
    for k, block in enumerate((p1, p2, p3)):
        put(r - k - 1, block, 0, 8)
    for k, block in enumerate((m1, m2, m3)):
        put(r + k + 1, block, 0, 8)
    put(r + 4, p4, 0, 4)
    put(r + 4, m4, 4, 8)

    gate_up = dot(norm_ref[...], w_ref[:, : 2 * HP], ((1,), (0,)))
    gate = gate_up[:, :HP]
    up = gate_up[:, HP:]
    d_hidden = HALF_STEP * dot(cot_ref[...], w_ref[:, 2 * HP :], ((1,), (0,)))
    sig = jax.nn.sigmoid(gate)
    hidden = (gate * sig * up).astype(jnp.bfloat16)
    d_gate = (d_hidden * up * sig * (1.0 + gate * (1.0 - sig))).astype(jnp.bfloat16)
    d_up = (d_hidden * gate * sig).astype(jnp.bfloat16)
    both = jnp.concatenate([d_gate, d_up], axis=1)
    part_ref[...] = dot(both, w_ref[:, : 2 * HP], ((1,), (1,))).astype(jnp.bfloat16)
    hidden_ref[...] = hidden
    keep_ref[...] = part_ref[half_rows(c), :]
    send_ref[...] = part_ref[half_rows(1 - c), :]


def turn_kernel(cot_ref, turned_ref):
    c = lax.axis_index("c")
    for z in range(NZ):
        block = cot_ref[:, z * 256 : (z + 1) * 256].T
        for y in range(NY):
            row = jnp.where(c == 0, z * 256 + y * 32, y * 256 + z * 32)
            rows = pl.ds(pl.multiple_of(row, 32), DROWS)
            turned_ref[rows, :] = block[y * 32 : (y + 1) * 32, :]


def down_kernel(turned_ref, hidden_ref, down_ref, staged_ref, sems):
    hidden = hidden_ref[...]
    copies = []
    for q in range(8):
        block = pl.ds(q * 256, 256)
        down = HALF_STEP * dot(turned_ref[block, :], hidden, ((1,), (0,)))
        staged_ref[block, :] = down.astype(jnp.bfloat16)
        copies.append(
            pltpu.make_async_copy(staged_ref.at[block, :], down_ref.at[block, :], sems.at[q])
        )
        copies[-1].start()
    for copy in copies:
        copy.wait()


def vmem_specs(count):
    return [pl.BlockSpec(memory_space=pltpu.VMEM)] * count


def small_call(kernel, out_shape, *operands):
    count = len(out_shape)
    return pl.pallas_call(
        kernel,
        out_shape=tuple(out_shape),
        in_specs=vmem_specs(len(operands)),
        out_specs=tuple(vmem_specs(count)),
        compiler_params=pltpu.CompilerParams(vmem_limit_bytes=SMALL_LIMIT),
    )(*operands)


def compute(normed, cotangent, blocks):
    half = jax.ShapeDtypeStruct((HALF, D), jnp.bfloat16)
    return pl.pallas_call(
        compute_kernel,
        out_shape=(
            half,
            half,
            jax.ShapeDtypeStruct((TOK, HP), jnp.bfloat16),
        ),
        in_specs=vmem_specs(2 + len(blocks)),
        out_specs=tuple(vmem_specs(3)),
        scratch_shapes=[
            pltpu.VMEM((D, 3 * HP), jnp.bfloat16),
            pltpu.VMEM((TOK, D), jnp.bfloat16),
        ],
        compiler_params=pltpu.CompilerParams(vmem_limit_bytes=VMEM_LIMIT),
    )(normed, cotangent, *blocks)


def turn(cotangent):
    return pl.pallas_call(
        turn_kernel,
        out_shape=jax.ShapeDtypeStruct((D, TOK), jnp.bfloat16),
        in_specs=vmem_specs(1),
        out_specs=vmem_specs(1)[0],
        compiler_params=pltpu.CompilerParams(vmem_limit_bytes=SMALL_LIMIT),
    )(cotangent)


def down_product(turned, hidden):
    return pl.pallas_call(
        down_kernel,
        out_shape=jax.ShapeDtypeStruct((D, HP), jnp.bfloat16),
        in_specs=vmem_specs(2),
        out_specs=pl.BlockSpec(memory_space=pltpu.HBM),
        scratch_shapes=[pltpu.VMEM((D, HP), jnp.bfloat16), pltpu.SemaphoreType.DMA((8,))],
        compiler_params=pltpu.CompilerParams(vmem_limit_bytes=DOWN_LIMIT),
    )(turned, hidden)


def pair_kernel(left_ref, right_ref, *out_refs):
    total = left_ref[...].astype(jnp.float32) + right_ref[...].astype(jnp.float32)
    rows = total.shape[0] // len(out_refs)
    for k, out in enumerate(out_refs):
        out[...] = total[k * rows : (k + 1) * rows].astype(jnp.bfloat16)


def final_kernel(x_ref, gain_ref, left1, right1, left2, right2, out_ref):
    gain = gain_ref[...]
    for k in range(4):
        rows = pl.ds(k * QUARTER, QUARTER)
        part = pl.ds(k % 2 * QUARTER, QUARTER)
        left, right = ((left1, right1), (left2, right2))[k // 2]
        value = x_ref[rows, :].astype(jnp.float32)
        inverse = lax.rsqrt(jnp.mean(value * value, axis=-1, keepdims=True) + EPSILON)
        normalized = value * inverse
        total = left[part, :].astype(jnp.float32) + right[part, :].astype(jnp.float32)
        scaled = total * gain
        mean = jnp.mean(scaled * normalized, axis=-1, keepdims=True)
        out_ref[rows, :] = (inverse * (scaled - normalized * mean)).astype(jnp.bfloat16)


def place_kernel(mine_ref, away_ref, out_ref, sems):
    c = lax.axis_index("c")
    copies = [
        pltpu.make_async_copy(ref, out_ref.at[half_rows(core), :], sems.at[k])
        for k, (core, ref) in enumerate(((c, mine_ref), (1 - c, away_ref)))
    ]
    for copy in copies:
        copy.start()
    for copy in copies:
        copy.wait()


def place(mine, away):
    return pl.pallas_call(
        place_kernel,
        out_shape=jax.ShapeDtypeStruct((TOK, D), jnp.bfloat16),
        in_specs=vmem_specs(2),
        out_specs=pl.BlockSpec(memory_space=pltpu.HBM),
        scratch_shapes=[pltpu.SemaphoreType.DMA((2,))],
        compiler_params=pltpu.CompilerParams(vmem_limit_bytes=SMALL_LIMIT),
    )(mine, away)


def sum_kernel(parts_ref, out_ref):
    total = parts_ref[0].astype(jnp.float32)
    for k in range(1, 8):
        total = total + parts_ref[k].astype(jnp.float32)
    out_ref[...] = total[:, : out_ref.shape[1]].astype(out_ref.dtype)


def with_partner(array, first):
    pairs = [
        (device_number(z, y, x, c), device_number(z, y, x ^ (1 if (c == 0) == first else 3), c))
        for z in range(NZ)
        for y in range(NY)
        for x in range(NX)
        for c in range(NC)
    ]
    return lax.ppermute(array, AXES, pairs)


def with_core(array):
    return lax.ppermute(array, "c", [(0, 1), (1, 0)])


def shards(inputs, gain, w_gate, w_up, w_down, cotangent):
    pad = ((0, 0), (0, HP - HU))
    packed = jnp.concatenate([jnp.pad(w, pad) for w in (w_gate, w_up, w_down.T)], axis=1)
    block = exchange(jnp.broadcast_to(packed[None], (8, DROWS, 3 * HP)), False)
    b0 = block.reshape(256, 3 * HP)
    p2 = ring(b0, 2)
    m2 = ring(b0, -2)
    p1 = ring(b0, 1)
    m1 = ring(b0, -1)
    p3 = ring(p2, 1)
    m3 = ring(m2, -1)
    p4 = ring(p2[:128], 2)
    m4 = ring(m2[128:], -2)

    row = gain.reshape(1, D)
    half = jax.ShapeDtypeStruct((HALF, D), jnp.bfloat16)
    normed, x_half = small_call(
        normalize_kernel, [jax.ShapeDtypeStruct((TOK, D), jnp.bfloat16), half], inputs, row
    )
    turned = turn(cotangent)
    keep, send, hidden = compute(normed, cotangent, (b0, p1, p2, p3, p4, m1, m2, m3, m4))
    other = with_core(send)
    down = down_product(turned, hidden)
    arrived = exchange(down.reshape(8, 256, HP), True)
    (line,) = small_call(sum_kernel, [jax.ShapeDtypeStruct((256, HP), jnp.bfloat16)], arrived)
    arrived = exchange(line.reshape(8, DROWS, HP), False)
    (total,) = small_call(sum_kernel, [jax.ShapeDtypeStruct((DROWS, HU), jnp.float32)], arrived)
    grad_down = total.T

    piece = jax.ShapeDtypeStruct((HALF // 2, D), jnp.bfloat16)
    chip1, chip2 = small_call(pair_kernel, [piece, piece], keep, other)
    got1 = with_partner(chip1, True)
    got2 = with_partner(chip2, True)
    (two1,) = small_call(pair_kernel, [piece], chip1, got1)
    far1 = with_partner(two1, False)
    (two2,) = small_call(pair_kernel, [piece], chip2, got2)
    far2 = with_partner(two2, False)
    (mine,) = small_call(final_kernel, [half], x_half, row, two1, far1, two2, far2)
    away = with_core(mine)
    whole = place(mine, away)
    return whole, grad_down


def solution(mesh):
    split = Mesh(mesh.devices.reshape(NZ, NY, NX, NC), AXES)
    in_specs = (P(FS, None), P(), P(FS, TP), P(FS, TP), P(TP, FS), P(FS, None))
    out_specs = (P(FS, None), P(TP, FS))
    return jax.shard_map(
        shards, mesh=split, in_specs=in_specs, out_specs=out_specs, check_vma=False
    )
```

```python
import jax
import jax.numpy as jnp
from jax import lax
from jax.experimental import pallas as pl
from jax.experimental.pallas import tpu as pltpu
from jax.sharding import Mesh
from jax.sharding import PartitionSpec as P


AXES = ("z", "y", "x", "c")
NZ, NY, NX, NC = 8, 8, 4, 2
FS = ("z", "y")
TP = ("x", "c")
EPSILON = 1e-06
HALF_STEP = 0.5
TOK = 384
D = 2048
HU = 352
HP = 384
DROWS = 32
HALF = TOK // NC
QUARTER = HALF // NX
VMEM_LIMIT = 28 * 2**20
SMALL_LIMIT = 6 * 2**20
DOWN_LIMIT = 16 * 2**20


def device_number(z, y, x, c):
    return ((z % NZ * NY + y % NY) * NX + x) * NC + c


def ring_pairs(step):
    return [
        (device_number(z, y, x, c), device_number(z + (1 - c) * step, y + c * step, x, c))
        for z in range(NZ)
        for y in range(NY)
        for x in range(NX)
        for c in range(NC)
    ]


def line_groups(along_ring):
    groups = []
    for x in range(NX):
        for c in range(NC):
            vary_z = (c == 0) == along_ring
            for fixed in range(8):
                groups.append(
                    [
                        device_number(k, fixed, x, c) if vary_z else device_number(fixed, k, x, c)
                        for k in range(8)
                    ]
                )
    return groups


def ring(array, step):
    return lax.ppermute(array, AXES, ring_pairs(step))


def exchange(array, along_ring):
    return lax.all_to_all(
        array, AXES, 0, 0, axis_index_groups=line_groups(along_ring), tiled=True
    )


def dot(left, right, dims):
    return lax.dot_general(left, right, (dims, ((), ())), preferred_element_type=jnp.float32)


def half_rows(core):
    return pl.ds(pl.multiple_of(core * HALF, 64), HALF)


def normalize_kernel(x_ref, gain_ref, xn_ref, half_ref):
    half_ref[...] = x_ref[half_rows(lax.axis_index("c")), :]
    gain = gain_ref[...]
    for k in range(6):
        rows = pl.ds(k * 64, 64)
        value = x_ref[rows, :].astype(jnp.float32)
        inverse = lax.rsqrt(jnp.mean(value * value, axis=-1, keepdims=True) + EPSILON)
        xn_ref[rows, :] = (value * inverse * gain).astype(jnp.bfloat16)


def block_rows(q, o):
    q = lax.rem(q + 16, 8)
    c = lax.axis_index("c")
    return pl.ds(pl.multiple_of(jnp.where(c == 0, q * 256 + o * 32, o * 256 + q * 32), 32), DROWS)


def ring_place():
    return jnp.where(lax.axis_index("c") == 0, lax.axis_index("z"), lax.axis_index("y"))


def early_kernel(
    norm_ref, cot_ref, b0, p1, p2, p3, m1, m2, m3, w_ref, gate_up_ref, d_hidden_ref
):
    r = ring_place()
    places = (r, r - 1, r - 2, r - 3, r + 1, r + 2, r + 3)
    for q, block in zip(places, (b0, p1, p2, p3, m1, m2, m3)):
        for o in range(8):
            w_ref[block_rows(q, o), :] = block[pl.ds(o * DROWS, DROWS), :]
    for o in range(8):
        w_ref[block_rows(r + 4, o), :] = jnp.zeros((DROWS, 3 * HP), jnp.bfloat16)
    gate_up_ref[...] = dot(norm_ref[...], w_ref[:, : 2 * HP], ((1,), (0,)))
    d_hidden_ref[...] = dot(cot_ref[...], w_ref[:, 2 * HP :], ((1,), (0,)))


def compute_kernel(
    w_in, gate_up_ref, d_hidden_ref, turned_x, turned_cot, p4, m4,
    keep_ref, send_ref, hidden_ref, w_ref, part_ref, last_ref,
):
    c = lax.axis_index("c")
    r = ring_place()
    last_ref[pl.ds(0, 128), :] = p4[...]
    last_ref[pl.ds(128, 128), :] = m4[...]
    for o in range(8):
        w_ref[block_rows(r + 4, o), :] = last_ref[pl.ds(o * DROWS, DROWS), :]

    last = pl.ds(pl.multiple_of(lax.rem(r + 4, 8) * 256, 256), 256)
    gate_up = gate_up_ref[...] + dot(turned_x[...], last_ref[:, : 2 * HP], ((0,), (0,)))
    gate = gate_up[:, :HP]
    up = gate_up[:, HP:]
    d_hidden = d_hidden_ref[...] + dot(turned_cot[last, :], last_ref[:, 2 * HP :], ((0,), (0,)))
    d_hidden = HALF_STEP * d_hidden
    sig = jax.nn.sigmoid(gate)
    hidden = (gate * sig * up).astype(jnp.bfloat16)
    d_gate = (d_hidden * up * sig * (1.0 + gate * (1.0 - sig))).astype(jnp.bfloat16)
    d_up = (d_hidden * gate * sig).astype(jnp.bfloat16)
    both = jnp.concatenate([d_gate, d_up], axis=1)
    part_ref[...] = dot(both, w_ref[:, : 2 * HP], ((1,), (1,))).astype(jnp.bfloat16)
    hidden_ref[...] = hidden
    keep_ref[...] = part_ref[half_rows(c), :]
    send_ref[...] = part_ref[half_rows(1 - c), :]


def turn_into(source_ref, turned_ref):
    c = lax.axis_index("c")
    for z in range(NZ):
        block = source_ref[:, z * 256 : (z + 1) * 256].T
        for y in range(NY):
            row = jnp.where(c == 0, z * 256 + y * 32, y * 256 + z * 32)
            rows = pl.ds(pl.multiple_of(row, 32), DROWS)
            turned_ref[rows, :] = block[y * 32 : (y + 1) * 32, :]


def turn_kernel(cot_ref, norm_ref, turned_ref, last_x_ref, all_ref):
    turn_into(cot_ref, turned_ref)
    turn_into(norm_ref, all_ref)
    last = pl.multiple_of(lax.rem(ring_place() + 4, 8) * 256, 256)
    last_x_ref[...] = all_ref[pl.ds(last, 256), :]


def down_kernel(turned_ref, hidden_ref, down_ref, staged_ref, sems):
    hidden = hidden_ref[...]
    copies = []
    for q in range(8):
        block = pl.ds(q * 256, 256)
        down = HALF_STEP * dot(turned_ref[block, :], hidden, ((1,), (0,)))
        staged_ref[block, :] = down.astype(jnp.bfloat16)
        copies.append(
            pltpu.make_async_copy(staged_ref.at[block, :], down_ref.at[block, :], sems.at[q])
        )
        copies[-1].start()
    for copy in copies:
        copy.wait()


def vmem_specs(count):
    return [pl.BlockSpec(memory_space=pltpu.VMEM)] * count


def small_call(kernel, out_shape, *operands):
    count = len(out_shape)
    return pl.pallas_call(
        kernel,
        out_shape=tuple(out_shape),
        in_specs=vmem_specs(len(operands)),
        out_specs=tuple(vmem_specs(count)),
        compiler_params=pltpu.CompilerParams(vmem_limit_bytes=SMALL_LIMIT),
    )(*operands)


def early(normed, cotangent, blocks):
    return pl.pallas_call(
        early_kernel,
        out_shape=(
            jax.ShapeDtypeStruct((D, 3 * HP), jnp.bfloat16),
            jax.ShapeDtypeStruct((TOK, 2 * HP), jnp.float32),
            jax.ShapeDtypeStruct((TOK, HP), jnp.float32),
        ),
        in_specs=vmem_specs(2 + len(blocks)),
        out_specs=tuple(vmem_specs(3)),
        compiler_params=pltpu.CompilerParams(vmem_limit_bytes=VMEM_LIMIT),
    )(normed, cotangent, *blocks)


def compute(*operands):
    half = jax.ShapeDtypeStruct((HALF, D), jnp.bfloat16)
    return pl.pallas_call(
        compute_kernel,
        out_shape=(
            half,
            half,
            jax.ShapeDtypeStruct((TOK, HP), jnp.bfloat16),
            jax.ShapeDtypeStruct((D, 3 * HP), jnp.bfloat16),
        ),
        in_specs=vmem_specs(len(operands)),
        out_specs=tuple(vmem_specs(4)),
        scratch_shapes=[
            pltpu.VMEM((TOK, D), jnp.bfloat16),
            pltpu.VMEM((256, 3 * HP), jnp.bfloat16),
        ],
        input_output_aliases={0: 3},
        compiler_params=pltpu.CompilerParams(vmem_limit_bytes=VMEM_LIMIT),
    )(*operands)


def turn(cotangent, normed):
    return pl.pallas_call(
        turn_kernel,
        out_shape=(
            jax.ShapeDtypeStruct((D, TOK), jnp.bfloat16),
            jax.ShapeDtypeStruct((256, TOK), jnp.bfloat16),
        ),
        in_specs=vmem_specs(2),
        out_specs=tuple(vmem_specs(2)),
        scratch_shapes=[pltpu.VMEM((D, TOK), jnp.bfloat16)],
        compiler_params=pltpu.CompilerParams(vmem_limit_bytes=SMALL_LIMIT),
    )(cotangent, normed)


def down_product(turned, hidden):
    return pl.pallas_call(
        down_kernel,
        out_shape=jax.ShapeDtypeStruct((D, HP), jnp.bfloat16),
        in_specs=vmem_specs(2),
        out_specs=pl.BlockSpec(memory_space=pltpu.HBM),
        scratch_shapes=[pltpu.VMEM((D, HP), jnp.bfloat16), pltpu.SemaphoreType.DMA((8,))],
        compiler_params=pltpu.CompilerParams(vmem_limit_bytes=DOWN_LIMIT),
    )(turned, hidden)


def pair_kernel(left_ref, right_ref, *out_refs):
    total = left_ref[...].astype(jnp.float32) + right_ref[...].astype(jnp.float32)
    rows = total.shape[0] // len(out_refs)
    for k, out in enumerate(out_refs):
        out[...] = total[k * rows : (k + 1) * rows].astype(jnp.bfloat16)


def final_kernel(x_ref, gain_ref, left1, right1, left2, right2, out_ref):
    gain = gain_ref[...]
    for k in range(4):
        rows = pl.ds(k * QUARTER, QUARTER)
        part = pl.ds(k % 2 * QUARTER, QUARTER)
        left, right = ((left1, right1), (left2, right2))[k // 2]
        value = x_ref[rows, :].astype(jnp.float32)
        inverse = lax.rsqrt(jnp.mean(value * value, axis=-1, keepdims=True) + EPSILON)
        normalized = value * inverse
        total = left[part, :].astype(jnp.float32) + right[part, :].astype(jnp.float32)
        scaled = total * gain
        mean = jnp.mean(scaled * normalized, axis=-1, keepdims=True)
        out_ref[rows, :] = (inverse * (scaled - normalized * mean)).astype(jnp.bfloat16)


def place_kernel(mine_ref, away_ref, out_ref, sems):
    c = lax.axis_index("c")
    copies = [
        pltpu.make_async_copy(ref, out_ref.at[half_rows(core), :], sems.at[k])
        for k, (core, ref) in enumerate(((c, mine_ref), (1 - c, away_ref)))
    ]
    for copy in copies:
        copy.start()
    for copy in copies:
        copy.wait()


def place(mine, away):
    return pl.pallas_call(
        place_kernel,
        out_shape=jax.ShapeDtypeStruct((TOK, D), jnp.bfloat16),
        in_specs=vmem_specs(2),
        out_specs=pl.BlockSpec(memory_space=pltpu.HBM),
        scratch_shapes=[pltpu.SemaphoreType.DMA((2,))],
        compiler_params=pltpu.CompilerParams(vmem_limit_bytes=SMALL_LIMIT),
    )(mine, away)


def sum_kernel(parts_ref, out_ref):
    total = parts_ref[0].astype(jnp.float32)
    for k in range(1, 8):
        total = total + parts_ref[k].astype(jnp.float32)
    out_ref[...] = total[:, : out_ref.shape[1]].astype(out_ref.dtype)


def with_partner(array, first):
    pairs = [
        (device_number(z, y, x, c), device_number(z, y, x ^ (1 if (c == 0) == first else 3), c))
        for z in range(NZ)
        for y in range(NY)
        for x in range(NX)
        for c in range(NC)
    ]
    return lax.ppermute(array, AXES, pairs)


def with_core(array):
    return lax.ppermute(array, "c", [(0, 1), (1, 0)])


def shards(inputs, gain, w_gate, w_up, w_down, cotangent):
    pad = ((0, 0), (0, HP - HU))
    packed = jnp.concatenate([jnp.pad(w, pad) for w in (w_gate, w_up, w_down.T)], axis=1)
    block = exchange(jnp.broadcast_to(packed[None], (8, DROWS, 3 * HP)), False)
    b0 = block.reshape(256, 3 * HP)
    p2 = ring(b0, 2)
    m2 = ring(b0, -2)
    p1 = ring(b0, 1)
    m1 = ring(b0, -1)
    p3 = ring(p2, 1)
    m3 = ring(m2, -1)
    p4 = ring(p2[:128], 2)
    m4 = ring(m2[128:], -2)

    row = gain.reshape(1, D)
    half = jax.ShapeDtypeStruct((HALF, D), jnp.bfloat16)
    normed, x_half = small_call(
        normalize_kernel, [jax.ShapeDtypeStruct((TOK, D), jnp.bfloat16), half], inputs, row
    )
    turned, last_x = turn(cotangent, normed)
    weights, gate_up, d_hidden = early(normed, cotangent, (b0, p1, p2, p3, m1, m2, m3))
    keep, send, hidden, _ = compute(weights, gate_up, d_hidden, last_x, turned, p4, m4)
    other = with_core(send)
    down = down_product(turned, hidden)
    arrived = exchange(down.reshape(8, 256, HP), True)
    (line,) = small_call(sum_kernel, [jax.ShapeDtypeStruct((256, HP), jnp.bfloat16)], arrived)
    arrived = exchange(line.reshape(8, DROWS, HP), False)
    (total,) = small_call(sum_kernel, [jax.ShapeDtypeStruct((DROWS, HU), jnp.float32)], arrived)
    grad_down = total.T

    piece = jax.ShapeDtypeStruct((HALF // 2, D), jnp.bfloat16)
    chip1, chip2 = small_call(pair_kernel, [piece, piece], keep, other)
    got1 = with_partner(chip1, True)
    got2 = with_partner(chip2, True)
    (two1,) = small_call(pair_kernel, [piece], chip1, got1)
    far1 = with_partner(two1, False)
    (two2,) = small_call(pair_kernel, [piece], chip2, got2)
    far2 = with_partner(two2, False)
    (mine,) = small_call(final_kernel, [half], x_half, row, two1, far1, two2, far2)
    away = with_core(mine)
    whole = place(mine, away)
    return whole, grad_down


def solution(mesh):
    split = Mesh(mesh.devices.reshape(NZ, NY, NX, NC), AXES)
    in_specs = (P(FS, None), P(), P(FS, TP), P(FS, TP), P(TP, FS), P(FS, None))
    out_specs = (P(FS, None), P(TP, FS))
    return jax.shard_map(
        shards, mesh=split, in_specs=in_specs, out_specs=out_specs, check_vma=False
    )
```

```python
import jax
import jax.numpy as jnp
from jax import lax
from jax.experimental import pallas as pl
from jax.experimental.pallas import tpu as pltpu
from jax.sharding import Mesh
from jax.sharding import PartitionSpec as P


AXES = ("z", "y", "x", "c")
NZ, NY, NX, NC = 8, 8, 4, 2
FS = ("z", "y")
TP = ("x", "c")
EPSILON = 1e-06
HALF_STEP = 0.5
TOK = 384
D = 2048
HU = 352
HP = 384
DROWS = 32
HALF = TOK // NC
VMEM_LIMIT = 28 * 2**20
SMALL_LIMIT = 6 * 2**20
DOWN_LIMIT = 16 * 2**20


def device_number(z, y, x, c):
    return ((z % NZ * NY + y % NY) * NX + x) * NC + c


def ring_pairs(step):
    return [
        (device_number(z, y, x, c), device_number(z + (1 - c) * step, y + c * step, x, c))
        for z in range(NZ)
        for y in range(NY)
        for x in range(NX)
        for c in range(NC)
    ]


def line_groups(along_ring):
    groups = []
    for x in range(NX):
        for c in range(NC):
            vary_z = (c == 0) == along_ring
            for fixed in range(8):
                groups.append(
                    [
                        device_number(k, fixed, x, c) if vary_z else device_number(fixed, k, x, c)
                        for k in range(8)
                    ]
                )
    return groups


def ring(array, step):
    return lax.ppermute(array, AXES, ring_pairs(step))


def exchange(array, along_ring):
    return lax.all_to_all(
        array, AXES, 0, 0, axis_index_groups=line_groups(along_ring), tiled=True
    )


def dot(left, right, dims):
    return lax.dot_general(left, right, (dims, ((), ())), preferred_element_type=jnp.float32)


def half_rows(core):
    return pl.ds(pl.multiple_of(core * HALF, 64), HALF)


def normalize_kernel(x_ref, gain_ref, xn_ref, half_ref):
    half_ref[...] = x_ref[half_rows(lax.axis_index("c")), :]
    gain = gain_ref[...]
    for k in range(6):
        rows = pl.ds(k * 64, 64)
        value = x_ref[rows, :].astype(jnp.float32)
        inverse = lax.rsqrt(jnp.mean(value * value, axis=-1, keepdims=True) + EPSILON)
        xn_ref[rows, :] = (value * inverse * gain).astype(jnp.bfloat16)


def block_rows(q, o):
    q = lax.rem(q + 16, 8)
    c = lax.axis_index("c")
    return pl.ds(pl.multiple_of(jnp.where(c == 0, q * 256 + o * 32, o * 256 + q * 32), 32), DROWS)


def ring_place():
    return jnp.where(lax.axis_index("c") == 0, lax.axis_index("z"), lax.axis_index("y"))


def early_kernel(
    norm_ref, cot_ref, b0, p1, p2, p3, m1, m2, m3, w_ref, gate_up_ref, d_hidden_ref
):
    r = ring_place()
    places = (r, r - 1, r - 2, r - 3, r + 1, r + 2, r + 3)
    for q, block in zip(places, (b0, p1, p2, p3, m1, m2, m3)):
        for o in range(8):
            w_ref[block_rows(q, o), :] = block[pl.ds(o * DROWS, DROWS), :]
    for o in range(8):
        w_ref[block_rows(r + 4, o), :] = jnp.zeros((DROWS, 3 * HP), jnp.bfloat16)
    gate_up_ref[...] = dot(norm_ref[...], w_ref[:, : 2 * HP], ((1,), (0,)))
    d_hidden_ref[...] = dot(cot_ref[...], w_ref[:, 2 * HP :], ((1,), (0,)))


def compute_kernel(
    w_in, gate_up_ref, d_hidden_ref, turned_x, turned_cot, p4, m4,
    keep_ref, send_ref, hidden_ref, w_ref, part_ref, last_ref, sum_ref, both_ref,
):
    c = lax.axis_index("c")
    r = ring_place()
    last_ref[pl.ds(0, 128), :] = p4[...]
    last_ref[pl.ds(128, 128), :] = m4[...]
    for o in range(8):
        w_ref[block_rows(r + 4, o), :] = last_ref[pl.ds(o * DROWS, DROWS), :]

    last = pl.ds(pl.multiple_of(lax.rem(r + 4, 8) * 256, 256), 256)
    sum_ref[:, : 2 * HP] = dot(turned_x[...], last_ref[:, : 2 * HP], ((0,), (0,)))
    sum_ref[:, 2 * HP :] = dot(turned_cot[last, :], last_ref[:, 2 * HP :], ((0,), (0,)))
    for k in range(TOK // 32):
        rows = pl.ds(k * 32, 32)
        gate = gate_up_ref[rows, :HP] + sum_ref[rows, :HP]
        up = gate_up_ref[rows, HP:] + sum_ref[rows, HP : 2 * HP]
        d_hidden = HALF_STEP * (d_hidden_ref[rows, :] + sum_ref[rows, 2 * HP :])
        sig = jax.nn.sigmoid(gate)
        hidden_ref[rows, :] = (gate * sig * up).astype(jnp.bfloat16)
        d_gate = d_hidden * up * sig * (1.0 + gate * (1.0 - sig))
        both_ref[rows, :HP] = d_gate.astype(jnp.bfloat16)
        both_ref[rows, HP:] = (d_hidden * gate * sig).astype(jnp.bfloat16)
    part_ref[...] = dot(both_ref[...], w_ref[:, : 2 * HP], ((1,), (1,))).astype(jnp.bfloat16)
    keep_ref[...] = part_ref[half_rows(c), :]
    send_ref[...] = part_ref[half_rows(1 - c), :]


def turn_into(source_ref, turned_ref):
    c = lax.axis_index("c")
    for z in range(NZ):
        block = source_ref[:, z * 256 : (z + 1) * 256].T
        for y in range(NY):
            row = jnp.where(c == 0, z * 256 + y * 32, y * 256 + z * 32)
            rows = pl.ds(pl.multiple_of(row, 32), DROWS)
            turned_ref[rows, :] = block[y * 32 : (y + 1) * 32, :]


def turn_kernel(cot_ref, norm_ref, turned_ref, last_x_ref, all_ref):
    turn_into(cot_ref, turned_ref)
    turn_into(norm_ref, all_ref)
    last = pl.multiple_of(lax.rem(ring_place() + 4, 8) * 256, 256)
    last_x_ref[...] = all_ref[pl.ds(last, 256), :]


def down_kernel(turned_ref, hidden_ref, down_ref, staged_ref, sems):
    hidden = hidden_ref[...]
    copies = []
    for q in range(8):
        block = pl.ds(q * 256, 256)
        down = HALF_STEP * dot(turned_ref[block, :], hidden, ((1,), (0,)))
        staged_ref[block, :] = down.astype(jnp.bfloat16)
        copies.append(
            pltpu.make_async_copy(staged_ref.at[block, :], down_ref.at[block, :], sems.at[q])
        )
        copies[-1].start()
    for copy in copies:
        copy.wait()


def vmem_specs(count):
    return [pl.BlockSpec(memory_space=pltpu.VMEM)] * count


def small_call(kernel, out_shape, *operands):
    count = len(out_shape)
    return pl.pallas_call(
        kernel,
        out_shape=tuple(out_shape),
        in_specs=vmem_specs(len(operands)),
        out_specs=tuple(vmem_specs(count)),
        compiler_params=pltpu.CompilerParams(vmem_limit_bytes=SMALL_LIMIT),
    )(*operands)


def early(normed, cotangent, blocks):
    return pl.pallas_call(
        early_kernel,
        out_shape=(
            jax.ShapeDtypeStruct((D, 3 * HP), jnp.bfloat16),
            jax.ShapeDtypeStruct((TOK, 2 * HP), jnp.float32),
            jax.ShapeDtypeStruct((TOK, HP), jnp.float32),
        ),
        in_specs=vmem_specs(2 + len(blocks)),
        out_specs=tuple(vmem_specs(3)),
        compiler_params=pltpu.CompilerParams(vmem_limit_bytes=VMEM_LIMIT),
    )(normed, cotangent, *blocks)


def compute(*operands):
    half = jax.ShapeDtypeStruct((HALF, D), jnp.bfloat16)
    return pl.pallas_call(
        compute_kernel,
        out_shape=(
            half,
            half,
            jax.ShapeDtypeStruct((TOK, HP), jnp.bfloat16),
            jax.ShapeDtypeStruct((D, 3 * HP), jnp.bfloat16),
        ),
        in_specs=vmem_specs(len(operands)),
        out_specs=tuple(vmem_specs(4)),
        scratch_shapes=[
            pltpu.VMEM((TOK, D), jnp.bfloat16),
            pltpu.VMEM((256, 3 * HP), jnp.bfloat16),
            pltpu.VMEM((TOK, 3 * HP), jnp.float32),
            pltpu.VMEM((TOK, 2 * HP), jnp.bfloat16),
        ],
        input_output_aliases={0: 3},
        compiler_params=pltpu.CompilerParams(vmem_limit_bytes=VMEM_LIMIT),
    )(*operands)


def turn(cotangent, normed):
    return pl.pallas_call(
        turn_kernel,
        out_shape=(
            jax.ShapeDtypeStruct((D, TOK), jnp.bfloat16),
            jax.ShapeDtypeStruct((256, TOK), jnp.bfloat16),
        ),
        in_specs=vmem_specs(2),
        out_specs=tuple(vmem_specs(2)),
        scratch_shapes=[pltpu.VMEM((D, TOK), jnp.bfloat16)],
        compiler_params=pltpu.CompilerParams(vmem_limit_bytes=SMALL_LIMIT),
    )(cotangent, normed)


def down_product(turned, hidden):
    return pl.pallas_call(
        down_kernel,
        out_shape=jax.ShapeDtypeStruct((D, HP), jnp.bfloat16),
        in_specs=vmem_specs(2),
        out_specs=pl.BlockSpec(memory_space=pltpu.HBM),
        scratch_shapes=[pltpu.VMEM((D, HP), jnp.bfloat16), pltpu.SemaphoreType.DMA((8,))],
        compiler_params=pltpu.CompilerParams(vmem_limit_bytes=DOWN_LIMIT),
    )(turned, hidden)


def pair_kernel(left_ref, right_ref, *out_refs):
    total = left_ref[...].astype(jnp.float32) + right_ref[...].astype(jnp.float32)
    rows = total.shape[0] // len(out_refs)
    for k, out in enumerate(out_refs):
        out[...] = total[k * rows : (k + 1) * rows].astype(jnp.bfloat16)


def inverse_kernel(x_ref, out_ref):
    for k in range(HALF // 16):
        rows = pl.ds(k * 16, 16)
        value = x_ref[rows, :].astype(jnp.float32)
        inverse = lax.rsqrt(jnp.mean(value * value, axis=-1, keepdims=True) + EPSILON)
        out_ref[rows, :] = jnp.broadcast_to(inverse, (16, 128))


def final_kernel(x_ref, inverse_ref, gain_ref, left1, right1, left2, right2, out_ref):
    for k in range(HALF // 16):
        rows = pl.ds(k * 16, 16)
        part = pl.ds(k * 16 % (HALF // 2), 16)
        left, right = ((left1, right1), (left2, right2))[k * 16 // (HALF // 2)]
        inverse = inverse_ref[rows, :1]
        normalized = x_ref[rows, :].astype(jnp.float32) * inverse
        total = left[part, :].astype(jnp.float32) + right[part, :].astype(jnp.float32)
        scaled = total * gain_ref[...]
        mean = jnp.mean(scaled * normalized, axis=-1, keepdims=True)
        out_ref[rows, :] = (inverse * (scaled - normalized * mean)).astype(jnp.bfloat16)


def place_kernel(mine_ref, away_ref, out_ref, sems):
    c = lax.axis_index("c")
    copies = [
        pltpu.make_async_copy(ref, out_ref.at[half_rows(core), :], sems.at[k])
        for k, (core, ref) in enumerate(((c, mine_ref), (1 - c, away_ref)))
    ]
    for copy in copies:
        copy.start()
    for copy in copies:
        copy.wait()


def place(mine, away):
    return pl.pallas_call(
        place_kernel,
        out_shape=jax.ShapeDtypeStruct((TOK, D), jnp.bfloat16),
        in_specs=vmem_specs(2),
        out_specs=pl.BlockSpec(memory_space=pltpu.HBM),
        scratch_shapes=[pltpu.SemaphoreType.DMA((2,))],
        compiler_params=pltpu.CompilerParams(vmem_limit_bytes=SMALL_LIMIT),
    )(mine, away)


def sum_kernel(parts_ref, out_ref):
    total = parts_ref[0].astype(jnp.float32)
    for k in range(1, 8):
        total = total + parts_ref[k].astype(jnp.float32)
    out_ref[...] = total[:, : out_ref.shape[1]].astype(out_ref.dtype)


def with_partner(array, first):
    pairs = [
        (device_number(z, y, x, c), device_number(z, y, x ^ (1 if (c == 0) == first else 3), c))
        for z in range(NZ)
        for y in range(NY)
        for x in range(NX)
        for c in range(NC)
    ]
    return lax.ppermute(array, AXES, pairs)


def with_core(array):
    return lax.ppermute(array, "c", [(0, 1), (1, 0)])


def shards(inputs, gain, w_gate, w_up, w_down, cotangent):
    pad = ((0, 0), (0, HP - HU))
    packed = jnp.concatenate([jnp.pad(w, pad) for w in (w_gate, w_up, w_down.T)], axis=1)
    block = exchange(jnp.broadcast_to(packed[None], (8, DROWS, 3 * HP)), False)
    b0 = block.reshape(256, 3 * HP)
    p2 = ring(b0, 2)
    m2 = ring(b0, -2)
    p1 = ring(b0, 1)
    m1 = ring(b0, -1)
    p3 = ring(p2, 1)
    m3 = ring(m2, -1)
    p4 = ring(p2[:128], 2)
    m4 = ring(m2[128:], -2)

    row = gain.reshape(1, D)
    half = jax.ShapeDtypeStruct((HALF, D), jnp.bfloat16)
    normed, x_half = small_call(
        normalize_kernel, [jax.ShapeDtypeStruct((TOK, D), jnp.bfloat16), half], inputs, row
    )
    turned, last_x = turn(cotangent, normed)
    weights, gate_up, d_hidden = early(normed, cotangent, (b0, p1, p2, p3, m1, m2, m3))
    keep, send, hidden, _ = compute(weights, gate_up, d_hidden, last_x, turned, p4, m4)
    other = with_core(send)
    down = down_product(turned, hidden)
    arrived = exchange(down.reshape(8, 256, HP), True)
    (line,) = small_call(sum_kernel, [jax.ShapeDtypeStruct((256, HP), jnp.bfloat16)], arrived)
    arrived = exchange(line.reshape(8, DROWS, HP), False)
    (total,) = small_call(sum_kernel, [jax.ShapeDtypeStruct((DROWS, HU), jnp.float32)], arrived)
    grad_down = total.T

    piece = jax.ShapeDtypeStruct((HALF // 2, D), jnp.bfloat16)
    chip1, chip2 = small_call(pair_kernel, [piece, piece], keep, other)
    got1 = with_partner(chip1, True)
    got2 = with_partner(chip2, True)
    (two1,) = small_call(pair_kernel, [piece], chip1, got1)
    far1 = with_partner(two1, False)
    (two2,) = small_call(pair_kernel, [piece], chip2, got2)
    far2 = with_partner(two2, False)
    (inverse,) = small_call(
        inverse_kernel, [jax.ShapeDtypeStruct((HALF, 128), jnp.float32)], x_half
    )
    (mine,) = small_call(final_kernel, [half], x_half, inverse, row, two1, far1, two2, far2)
    away = with_core(mine)
    whole = place(mine, away)
    return whole, grad_down


def solution(mesh):
    split = Mesh(mesh.devices.reshape(NZ, NY, NX, NC), AXES)
    in_specs = (P(FS, None), P(), P(FS, TP), P(FS, TP), P(TP, FS), P(FS, None))
    out_specs = (P(FS, None), P(TP, FS))
    return jax.shard_map(
        shards, mesh=split, in_specs=in_specs, out_specs=out_specs, check_vma=False
    )
```

```python
import jax
import jax.numpy as jnp
from jax import lax
from jax.experimental import pallas as pl
from jax.experimental.pallas import tpu as pltpu
from jax.sharding import Mesh
from jax.sharding import PartitionSpec as P


AXES = ("z", "y", "x", "c")
NZ, NY, NX, NC = 8, 8, 4, 2
FS = ("z", "y")
TP = ("x", "c")
EPSILON = 1e-06
HALF_STEP = 0.5
TOK = 384
D = 2048
HU = 352
HP = 384
DROWS = 32
HALF = TOK // NC
QUARTER = HALF // NX
VMEM_LIMIT = 28 * 2**20
SMALL_LIMIT = 6 * 2**20
DOWN_LIMIT = 16 * 2**20


def device_number(z, y, x, c):
    return ((z % NZ * NY + y % NY) * NX + x) * NC + c


def ring_pairs(step):
    return [
        (device_number(z, y, x, c), device_number(z + (1 - c) * step, y + c * step, x, c))
        for z in range(NZ)
        for y in range(NY)
        for x in range(NX)
        for c in range(NC)
    ]


def line_groups(along_ring):
    groups = []
    for x in range(NX):
        for c in range(NC):
            vary_z = (c == 0) == along_ring
            for fixed in range(8):
                groups.append(
                    [
                        device_number(k, fixed, x, c) if vary_z else device_number(fixed, k, x, c)
                        for k in range(8)
                    ]
                )
    return groups


def ring(array, step):
    return lax.ppermute(array, AXES, ring_pairs(step))


def exchange(array, along_ring):
    return lax.all_to_all(
        array, AXES, 0, 0, axis_index_groups=line_groups(along_ring), tiled=True
    )


def dot(left, right, dims):
    return lax.dot_general(left, right, (dims, ((), ())), preferred_element_type=jnp.float32)


def half_rows(core):
    return pl.ds(pl.multiple_of(core * HALF, 64), HALF)


def normalize_kernel(x_ref, gain_ref, xn_ref, half_ref):
    half_ref[...] = x_ref[half_rows(lax.axis_index("c")), :]
    gain = gain_ref[...]
    for k in range(6):
        rows = pl.ds(k * 64, 64)
        value = x_ref[rows, :].astype(jnp.float32)
        inverse = lax.rsqrt(jnp.mean(value * value, axis=-1, keepdims=True) + EPSILON)
        xn_ref[rows, :] = (value * inverse * gain).astype(jnp.bfloat16)


def block_rows(q, o):
    q = lax.rem(q + 16, 8)
    c = lax.axis_index("c")
    return pl.ds(pl.multiple_of(jnp.where(c == 0, q * 256 + o * 32, o * 256 + q * 32), 32), DROWS)


def ring_place():
    return jnp.where(lax.axis_index("c") == 0, lax.axis_index("z"), lax.axis_index("y"))


def early_kernel(
    norm_ref, cot_ref, b0, p1, p2, p3, m1, m2, m3, w_ref, gate_up_ref, d_hidden_ref
):
    r = ring_place()
    places = (r, r - 1, r - 2, r - 3, r + 1, r + 2, r + 3)
    for q, block in zip(places, (b0, p1, p2, p3, m1, m2, m3)):
        for o in range(8):
            w_ref[block_rows(q, o), :] = block[pl.ds(o * DROWS, DROWS), :]
    for o in range(8):
        w_ref[block_rows(r + 4, o), :] = jnp.zeros((DROWS, 3 * HP), jnp.bfloat16)
    gate_up_ref[...] = dot(norm_ref[...], w_ref[:, : 2 * HP], ((1,), (0,)))
    d_hidden_ref[...] = dot(cot_ref[...], w_ref[:, 2 * HP :], ((1,), (0,)))


def compute_kernel(
    w_in, gate_up_ref, d_hidden_ref, turned_x, turned_cot, p4, m4,
    keep_ref, send_ref, hidden_ref, w_ref, part_ref, last_ref,
):
    c = lax.axis_index("c")
    r = ring_place()
    last_ref[pl.ds(0, 128), :] = p4[...]
    last_ref[pl.ds(128, 128), :] = m4[...]
    for o in range(8):
        w_ref[block_rows(r + 4, o), :] = last_ref[pl.ds(o * DROWS, DROWS), :]

    last = pl.ds(pl.multiple_of(lax.rem(r + 4, 8) * 256, 256), 256)
    gate_up = gate_up_ref[...] + dot(turned_x[...], last_ref[:, : 2 * HP], ((0,), (0,)))
    gate = gate_up[:, :HP]
    up = gate_up[:, HP:]
    d_hidden = d_hidden_ref[...] + dot(turned_cot[last, :], last_ref[:, 2 * HP :], ((0,), (0,)))
    d_hidden = HALF_STEP * d_hidden
    sig = jax.nn.sigmoid(gate)
    hidden = (gate * sig * up).astype(jnp.bfloat16)
    d_gate = (d_hidden * up * sig * (1.0 + gate * (1.0 - sig))).astype(jnp.bfloat16)
    d_up = (d_hidden * gate * sig).astype(jnp.bfloat16)
    both = jnp.concatenate([d_gate, d_up], axis=1)
    part_ref[...] = dot(both, w_ref[:, : 2 * HP], ((1,), (1,))).astype(jnp.bfloat16)
    hidden_ref[...] = hidden
    keep_ref[...] = part_ref[half_rows(c), :]
    send_ref[...] = part_ref[half_rows(1 - c), :]


def turn_into(source_ref, turned_ref):
    c = lax.axis_index("c")
    for z in range(NZ):
        block = source_ref[:, z * 256 : (z + 1) * 256].T
        for y in range(NY):
            row = jnp.where(c == 0, z * 256 + y * 32, y * 256 + z * 32)
            rows = pl.ds(pl.multiple_of(row, 32), DROWS)
            turned_ref[rows, :] = block[y * 32 : (y + 1) * 32, :]


def turn_kernel(cot_ref, norm_ref, turned_ref, last_x_ref, all_ref):
    turn_into(cot_ref, turned_ref)
    turn_into(norm_ref, all_ref)
    last = pl.multiple_of(lax.rem(ring_place() + 4, 8) * 256, 256)
    last_x_ref[...] = all_ref[pl.ds(last, 256), :]


def down_kernel(turned_ref, hidden_ref, down_ref, staged_ref, sems):
    hidden = hidden_ref[...]
    copies = []
    for q in range(8):
        block = pl.ds(q * 256, 256)
        down = HALF_STEP * dot(turned_ref[block, :], hidden, ((1,), (0,)))
        staged_ref[block, :] = down.astype(jnp.bfloat16)
        copies.append(
            pltpu.make_async_copy(staged_ref.at[block, :], down_ref.at[block, :], sems.at[q])
        )
        copies[-1].start()
    for copy in copies:
        copy.wait()


def vmem_specs(count):
    return [pl.BlockSpec(memory_space=pltpu.VMEM)] * count


def small_call(kernel, out_shape, *operands):
    count = len(out_shape)
    return pl.pallas_call(
        kernel,
        out_shape=tuple(out_shape),
        in_specs=vmem_specs(len(operands)),
        out_specs=tuple(vmem_specs(count)),
        compiler_params=pltpu.CompilerParams(vmem_limit_bytes=SMALL_LIMIT),
    )(*operands)


def early(normed, cotangent, blocks):
    return pl.pallas_call(
        early_kernel,
        out_shape=(
            jax.ShapeDtypeStruct((D, 3 * HP), jnp.bfloat16),
            jax.ShapeDtypeStruct((TOK, 2 * HP), jnp.float32),
            jax.ShapeDtypeStruct((TOK, HP), jnp.float32),
        ),
        in_specs=vmem_specs(2 + len(blocks)),
        out_specs=tuple(vmem_specs(3)),
        compiler_params=pltpu.CompilerParams(vmem_limit_bytes=VMEM_LIMIT),
    )(normed, cotangent, *blocks)


def compute(*operands):
    half = jax.ShapeDtypeStruct((HALF, D), jnp.bfloat16)
    return pl.pallas_call(
        compute_kernel,
        out_shape=(
            half,
            half,
            jax.ShapeDtypeStruct((TOK, HP), jnp.bfloat16),
            jax.ShapeDtypeStruct((D, 3 * HP), jnp.bfloat16),
        ),
        in_specs=vmem_specs(len(operands)),
        out_specs=tuple(vmem_specs(4)),
        scratch_shapes=[
            pltpu.VMEM((TOK, D), jnp.bfloat16),
            pltpu.VMEM((256, 3 * HP), jnp.bfloat16),
        ],
        input_output_aliases={0: 3},
        compiler_params=pltpu.CompilerParams(vmem_limit_bytes=VMEM_LIMIT),
    )(*operands)


def turn(cotangent, normed):
    return pl.pallas_call(
        turn_kernel,
        out_shape=(
            jax.ShapeDtypeStruct((D, TOK), jnp.bfloat16),
            jax.ShapeDtypeStruct((256, TOK), jnp.bfloat16),
        ),
        in_specs=vmem_specs(2),
        out_specs=tuple(vmem_specs(2)),
        scratch_shapes=[pltpu.VMEM((D, TOK), jnp.bfloat16)],
        compiler_params=pltpu.CompilerParams(vmem_limit_bytes=SMALL_LIMIT),
    )(cotangent, normed)


def down_product(turned, hidden):
    return pl.pallas_call(
        down_kernel,
        out_shape=jax.ShapeDtypeStruct((D, HP), jnp.bfloat16),
        in_specs=vmem_specs(2),
        out_specs=pl.BlockSpec(memory_space=pltpu.HBM),
        scratch_shapes=[pltpu.VMEM((D, HP), jnp.bfloat16), pltpu.SemaphoreType.DMA((8,))],
        compiler_params=pltpu.CompilerParams(vmem_limit_bytes=DOWN_LIMIT),
    )(turned, hidden)


def pair_kernel(left_ref, right_ref, *out_refs):
    total = left_ref[...].astype(jnp.float32) + right_ref[...].astype(jnp.float32)
    rows = total.shape[0] // len(out_refs)
    for k, out in enumerate(out_refs):
        out[...] = total[k * rows : (k + 1) * rows].astype(jnp.bfloat16)


def inverse_kernel(x_ref, out_ref):
    for k in range(4):
        rows = pl.ds(k * QUARTER, QUARTER)
        value = x_ref[rows, :].astype(jnp.float32)
        inverse = lax.rsqrt(jnp.mean(value * value, axis=-1, keepdims=True) + EPSILON)
        out_ref[rows, :] = jnp.broadcast_to(inverse, (QUARTER, 128))


def final_kernel(x_ref, inverse_ref, gain_ref, left1, right1, left2, right2, out_ref):
    gain = gain_ref[...]
    for k in range(4):
        rows = pl.ds(k * QUARTER, QUARTER)
        part = pl.ds(k % 2 * QUARTER, QUARTER)
        left, right = ((left1, right1), (left2, right2))[k // 2]
        inverse = inverse_ref[rows, :1]
        normalized = x_ref[rows, :].astype(jnp.float32) * inverse
        total = left[part, :].astype(jnp.float32) + right[part, :].astype(jnp.float32)
        scaled = total * gain
        mean = jnp.mean(scaled * normalized, axis=-1, keepdims=True)
        out_ref[rows, :] = (inverse * (scaled - normalized * mean)).astype(jnp.bfloat16)


def place_kernel(mine_ref, away_ref, out_ref, sems):
    c = lax.axis_index("c")
    copies = [
        pltpu.make_async_copy(ref, out_ref.at[half_rows(core), :], sems.at[k])
        for k, (core, ref) in enumerate(((c, mine_ref), (1 - c, away_ref)))
    ]
    for copy in copies:
        copy.start()
    for copy in copies:
        copy.wait()


def place(mine, away):
    return pl.pallas_call(
        place_kernel,
        out_shape=jax.ShapeDtypeStruct((TOK, D), jnp.bfloat16),
        in_specs=vmem_specs(2),
        out_specs=pl.BlockSpec(memory_space=pltpu.HBM),
        scratch_shapes=[pltpu.SemaphoreType.DMA((2,))],
        compiler_params=pltpu.CompilerParams(vmem_limit_bytes=SMALL_LIMIT),
    )(mine, away)


def sum_kernel(parts_ref, out_ref):
    total = parts_ref[0].astype(jnp.float32)
    for k in range(1, 8):
        total = total + parts_ref[k].astype(jnp.float32)
    out_ref[...] = total[:, : out_ref.shape[1]].astype(out_ref.dtype)


def with_partner(array, first):
    pairs = [
        (device_number(z, y, x, c), device_number(z, y, x ^ (1 if (c == 0) == first else 3), c))
        for z in range(NZ)
        for y in range(NY)
        for x in range(NX)
        for c in range(NC)
    ]
    return lax.ppermute(array, AXES, pairs)


def with_core(array):
    return lax.ppermute(array, "c", [(0, 1), (1, 0)])


def shards(inputs, gain, w_gate, w_up, w_down, cotangent):
    pad = ((0, 0), (0, HP - HU))
    packed = jnp.concatenate([jnp.pad(w, pad) for w in (w_gate, w_up, w_down.T)], axis=1)
    block = exchange(jnp.broadcast_to(packed[None], (8, DROWS, 3 * HP)), False)
    b0 = block.reshape(256, 3 * HP)
    p2 = ring(b0, 2)
    m2 = ring(b0, -2)
    p1 = ring(b0, 1)
    m1 = ring(b0, -1)
    p3 = ring(p2, 1)
    m3 = ring(m2, -1)
    p4 = ring(p2[:128], 2)
    m4 = ring(m2[128:], -2)

    row = gain.reshape(1, D)
    half = jax.ShapeDtypeStruct((HALF, D), jnp.bfloat16)
    normed, x_half = small_call(
        normalize_kernel, [jax.ShapeDtypeStruct((TOK, D), jnp.bfloat16), half], inputs, row
    )
    turned, last_x = turn(cotangent, normed)
    weights, gate_up, d_hidden = early(normed, cotangent, (b0, p1, p2, p3, m1, m2, m3))
    keep, send, hidden, _ = compute(weights, gate_up, d_hidden, last_x, turned, p4, m4)
    other = with_core(send)
    down = down_product(turned, hidden)
    arrived = exchange(down.reshape(8, 256, HP), True)
    (line,) = small_call(sum_kernel, [jax.ShapeDtypeStruct((256, HP), jnp.bfloat16)], arrived)
    arrived = exchange(line.reshape(8, DROWS, HP), False)
    (total,) = small_call(sum_kernel, [jax.ShapeDtypeStruct((DROWS, HU), jnp.float32)], arrived)
    grad_down = total.T

    piece = jax.ShapeDtypeStruct((HALF // 2, D), jnp.bfloat16)
    chip1, chip2 = small_call(pair_kernel, [piece, piece], keep, other)
    got1 = with_partner(chip1, True)
    got2 = with_partner(chip2, True)
    (two1,) = small_call(pair_kernel, [piece], chip1, got1)
    far1 = with_partner(two1, False)
    (two2,) = small_call(pair_kernel, [piece], chip2, got2)
    far2 = with_partner(two2, False)
    (inverse,) = small_call(
        inverse_kernel, [jax.ShapeDtypeStruct((HALF, 128), jnp.float32)], x_half
    )
    (mine,) = small_call(final_kernel, [half], x_half, inverse, row, two1, far1, two2, far2)
    away = with_core(mine)
    whole = place(mine, away)
    return whole, grad_down


def solution(mesh):
    split = Mesh(mesh.devices.reshape(NZ, NY, NX, NC), AXES)
    in_specs = (P(FS, None), P(), P(FS, TP), P(FS, TP), P(TP, FS), P(FS, None))
    out_specs = (P(FS, None), P(TP, FS))
    return jax.shard_map(
        shards, mesh=split, in_specs=in_specs, out_specs=out_specs, check_vma=False
    )
```
